32 devices in a mesh: sp: 8 (over z, x), tp: 4 (over y, core).
Axes of the slice: x: 2, y: 2, z: 4, core: 2. Of those that a mesh axis runs over, the one named last changes fastest.
Arguments:
- residual: bfloat16 [1024, 2048], P(('sp', 'tp')), may hold values from -6 to 6
- query_first: bfloat16 [1024, 1024], P('sp', 'tp'), may hold values from -200 to 200
- key_first: bfloat16 [1024, 1024], P('sp', 'tp'), may hold values from -200 to 200
- query_second: bfloat16 [1024, 1024], P('sp', 'tp'), may hold values from -200 to 200
- key_second: bfloat16 [1024, 1024], P('sp', 'tp'), may hold values from -200 to 200
- values: bfloat16 [1024, 2048], P('sp', 'tp'), may hold values from -6 to 6
- lambda_weight: float32 [16], P('tp'), may hold values from 0.3 to 0.8
- head_gain: float32 [128], replicated, may hold values from 0.1 to 1.9
- out_weight: bfloat16 [2048, 2048], P('sp', 'tp'), may hold values from -0.125 to 0.125
- norm_gain: float32 [2048], replicated, may hold values from 0.1 to 1.9
- gate_weight: bfloat16 [2048, 5632], P(None, 'tp'), may hold values from -0.125 to 0.125
- up_weight: bfloat16 [2048, 5632], P(None, 'tp'), may hold values from -0.125 to 0.125
- down_weight: bfloat16 [2048, 5632], P('sp', 'tp'), may hold values from -0.078125 to 0.078125
Outputs:
- layer_out: bfloat16 [1024, 2048], P(('sp', 'tp'))
The draws below stay inside these ranges and needn't reach their ends.
All inputs are finite; a program needn't handle non-finite values.
Results may differ from the reference program's by a relative error of at most 0.017.
Values may be sent and summed in bfloat16 or wider, within the bound.
A program may use at most 128 MiB of HBM per device.

```python
import jax
import jax.numpy as jnp
from jax import lax

D = 2048
HEADS = 16
HD = 64
VD = 128
FF = 5632
TOKENS = 1024
N_TP = 4


def plant_pair(key, which):
    spread = 1.32
    key_rows = jax.random.normal(jax.random.fold_in(key, 101 + which), (TOKENS, HEADS * HD), jnp.float32) * spread
    key_rows = jnp.clip(key_rows, -6.0 * spread, 6.0 * spread)
    queries = jax.random.normal(jax.random.fold_in(key, 201 + which), (TOKENS, HEADS * HD), jnp.float32) * spread
    queries = jnp.clip(queries, -6.0 * spread, 6.0 * spread)
    return (queries, key_rows)


def draw_query_first(key, part):
    return plant_pair(key, 0)[0].astype(jnp.bfloat16)


def draw_key_first(key, part):
    return plant_pair(key, 0)[1].astype(jnp.bfloat16)


def draw_query_second(key, part):
    return plant_pair(key, 1)[0].astype(jnp.bfloat16)


def draw_key_second(key, part):
    return plant_pair(key, 1)[1].astype(jnp.bfloat16)


def shard_levels(rng, shape, cuts, low, high):
    def one(axis_at, blocks):
        steps = jax.random.uniform(jax.random.fold_in(jax.random.fold_in(rng, 6), axis_at), (blocks,), jnp.float32, low / len(cuts), high / len(cuts))
        return jnp.repeat(jnp.exp(steps), shape[axis_at] // blocks).reshape((-1,) + (1,) * (len(shape) - axis_at - 1))

    level = one(*cuts[0])
    for cut in cuts[1:]:
        level = level * one(*cut)
    return level


def normal_values(stream_key, extent, deviation, reach, cuts=(), held_as=jnp.bfloat16):
    loudness = shard_levels(stream_key, extent, cuts, -0.22, 0.18) if cuts else 1.0
    values = jax.random.normal(stream_key, extent, jnp.float32) * deviation * loudness
    return jnp.minimum(jnp.maximum(values, -reach), reach).astype(held_as)


def setup_inputs(seed: int = 0) -> dict:
    arg_keys = jax.random.split(jax.random.key(seed), 14)
    residual = normal_values(arg_keys[0], (TOKENS, D), 1.0, 6.0, ((0, 32),))
    query_first = draw_query_first(jax.random.fold_in(arg_keys[13], 71), 0)
    key_first = draw_key_first(jax.random.fold_in(arg_keys[13], 71), 0)
    query_second = draw_query_second(jax.random.fold_in(arg_keys[13], 71), 0)
    key_second = draw_key_second(jax.random.fold_in(arg_keys[13], 71), 0)
    values = normal_values(arg_keys[5], (TOKENS, HEADS * VD), 1.0, 6.0, ((0, 8), (1, 4)))
    lambda_weight = jnp.clip(0.3 + 0.5 * jax.random.uniform(arg_keys[6], (HEADS,), jnp.float32) ** shard_levels(arg_keys[6], (HEADS,), ((0, 4),), -0.2, 0.2), 0.3, 0.8)
    head_gain = jnp.clip(1.0 + 0.18 * jax.random.normal(arg_keys[7], (VD,), jnp.float32), 0.1, 1.9)
    out_weight = normal_values(arg_keys[8], (D, HEADS * VD), (HEADS * VD) ** -0.5, 0.125, ((0, 8), (1, 4)))
    norm_gain = jnp.clip(1.0 + 0.18 * jax.random.normal(arg_keys[9], (D,), jnp.float32), 0.1, 1.9)
    gate_weight = normal_values(arg_keys[10], (D, FF), D ** -0.5, 0.125, ((1, 4),))
    up_weight = normal_values(arg_keys[11], (D, FF), D ** -0.5, 0.125, ((1, 4),))
    down_weight = normal_values(arg_keys[12], (D, FF), FF ** -0.5, 0.078125, ((0, 8), (1, 4)))
    return {"residual": residual, "query_first": query_first, "key_first": key_first, "query_second": query_second, "key_second": key_second, "values": values, "lambda_weight": lambda_weight, "head_gain": head_gain, "out_weight": out_weight, "norm_gain": norm_gain, "gate_weight": gate_weight, "up_weight": up_weight, "down_weight": down_weight}


epsilon = 1e-06

def one_map(queries, key_rows, value_rows):
    scores = jnp.dot(queries, key_rows.T, preferred_element_type=jnp.float32) * queries.shape[-1] ** (-0.5)
    shifted = jnp.exp(scores - lax.optimization_barrier(jnp.max(scores, axis=-1, keepdims=True)))
    totals = lax.optimization_barrier(jnp.sum(shifted, axis=-1, keepdims=True))
    product = jnp.dot(shifted.astype(jnp.bfloat16), value_rows, preferred_element_type=jnp.float32)
    return product / totals

def attend_head(inputs, head_gain):
    query_one, key_one, query_two, key_two, value_rows, weight = inputs
    first_map = one_map(query_one, key_one, value_rows)
    second_map = one_map(query_two, key_two, value_rows)
    difference = first_map - weight * second_map
    scaled = difference * lax.rsqrt(lax.optimization_barrier(jnp.mean(difference * difference, axis=-1, keepdims=True)) + epsilon)
    return (scaled * head_gain).astype(jnp.bfloat16)

def reference(residual, query_first, key_first, query_second, key_second, values, lambda_weight, head_gain, out_weight, norm_gain, gate_weight, up_weight, down_weight):
    length = query_first.shape[0]

    def split_heads(array, entries):
        return array.reshape(length, HEADS, entries).transpose(1, 0, 2)
    stacked = (split_heads(query_first, HD), split_heads(key_first, HD), split_heads(query_second, HD), split_heads(key_second, HD), split_heads(values, VD), lambda_weight)
    heads_out = lax.map(lambda inputs: attend_head(inputs, head_gain), stacked)
    attended = heads_out.transpose(1, 0, 2).reshape(length, HEADS * VD)
    group_width = HEADS * VD // N_TP
    projected = jnp.zeros((length, D), jnp.float32)
    for member in range(N_TP):
        columns = slice(member * group_width, (member + 1) * group_width)
        partial_value = lax.dot_general(attended[:, columns], out_weight[:, columns], (((1,), (1,)), ((), ())), preferred_element_type=jnp.float32)
        projected = projected + lax.optimization_barrier(partial_value.astype(jnp.bfloat16)).astype(jnp.float32)
    after_attention = (residual.astype(jnp.float32) + projected).astype(jnp.bfloat16)
    stream = after_attention.astype(jnp.float32)
    normed = (stream * lax.rsqrt(lax.optimization_barrier(jnp.mean(stream * stream, axis=-1, keepdims=True)) + epsilon) * norm_gain).astype(jnp.bfloat16)
    hidden_width = FF // N_TP
    feed_sum = jnp.zeros((length, D), jnp.float32)
    for member in range(N_TP):
        columns = slice(member * hidden_width, (member + 1) * hidden_width)
        gate_part = jnp.dot(normed, gate_weight[:, columns], preferred_element_type=jnp.float32)
        up_part = jnp.dot(normed, up_weight[:, columns], preferred_element_type=jnp.float32)
        hidden = (jax.nn.silu(gate_part) * up_part).astype(jnp.bfloat16)
        partial_value = lax.dot_general(hidden, down_weight[:, columns], (((1,), (1,)), ((), ())), preferred_element_type=jnp.float32)
        feed_sum = feed_sum + lax.optimization_barrier(partial_value.astype(jnp.bfloat16)).astype(jnp.float32)
    return (stream + feed_sum).astype(jnp.bfloat16)
```

```python
import functools

import jax
import jax.numpy as jnp
from jax import lax
from jax.experimental import pallas as pl
from jax.experimental.pallas import tpu as pltpu
from jax.sharding import PartitionSpec as P

epsilon = 1e-06
ROWS_ROWS = (((1,), (1,)), ((), ()))
CHUNKS = 4
X_FIRST = 1
PIECES = 2


def split_sp(size):
    inner = 1
    while (2 * inner) * (2 * inner) <= size:
        inner *= 2
    return size // inner, inner


def kernel(
    Z,
    X,
    T,
    C,
    heads,
    residual,
    q_one,
    k_one,
    q_two,
    k_two,
    values,
    lam,
    head_gain,
    out_weight,
    norm_gain,
    gate_weight,
    up_weight,
    down_weight,
    result,
    stage,
    value_stage,
    q_pack,
    k_pack,
    q_all,
    k_all,
    v_all,
    outw,
    downw,
    gate,
    up,
    att_out,
    att,
    res,
    core_out,
    core_in,
    y_out,
    y_in,
    own_sum,
    full,
    normed,
    hidden,
    owner_out,
    owner_in,
    local_sem,
    send_sem,
    recv_sem,
):
    f32, bf16 = jnp.float32, jnp.bfloat16
    scope = jax.named_scope
    s = lax.axis_index("sp")
    t = lax.axis_index("tp")
    z, x = s // X, s % X
    sp = Z * X
    Zh = Z // 2
    G = Zh * X
    half = z // Zh
    other = 1 - half
    zl = z % Zh
    j = zl * X + x
    mate = other * G + j
    Y = T // 2
    y, c = t // 2, t % 2
    tokens = q_one.shape[0]
    piece = tokens // T
    h = s % heads
    first = s - h
    quarter = full.shape[2] // 4

    def z_at(d):
        return (half * Zh + (zl + d) % Zh) * X + x

    def zl_from(d):
        return (zl - d + Zh) % Zh

    def x_at(d):
        return z * X + (x + d) % X

    def x_from(d):
        return (x - d + X) % X

    def t_of(yy, cc):
        return yy * 2 + cc

    def device(sp_at, tp_at):
        return {"sp": sp_at, "tp": tp_at}

    barrier = pltpu.get_barrier_semaphore()
    peers = [((s + d) % sp, t) for d in range(1, sp)]
    peers += [(s, (t + d) % T) for d in range(1, T)]
    peers += [(mate, (t + d) % T) for d in range(1, T)]
    for sp_at, tp_at in peers:
        pl.semaphore_signal(
            barrier, inc=1, device_id=device(sp_at, tp_at), device_id_type=pl.DeviceIdType.MESH
        )

    moves = [
        (k_one, stage.at[0]),
        (k_two, stage.at[1]),
        (q_one, stage.at[2]),
        (q_two, stage.at[3]),
        (values, value_stage),
        (out_weight, outw.at[j]),
        (down_weight, downw.at[j]),
        (gate_weight, gate),
        (up_weight, up),
    ]
    moving = [
        pltpu.make_async_copy(src, dst, local_sem.at[i]) for i, (src, dst) in enumerate(moves)
    ]
    for copy in moving:
        copy.start()

    names = {}
    sends = []

    def slot(name):
        return names.setdefault(name, len(names))

    def send(src, dst, name, sp_at, tp_at):
        k = slot(name)
        pltpu.make_async_remote_copy(
            src_ref=src, dst_ref=dst, send_sem=send_sem.at[k], recv_sem=recv_sem.at[k],
            device_id=device(sp_at, tp_at), device_id_type=pl.DeviceIdType.MESH,
        ).start()

    def wait(ref, name):
        k = slot(name)
        return pltpu.make_async_remote_copy(
            src_ref=ref, dst_ref=ref, send_sem=send_sem.at[k], recv_sem=recv_sem.at[k],
            device_id=device(s, t), device_id_type=pl.DeviceIdType.MESH,
        )

    def arrive(ref, name, same=True):
        wait(ref, name).wait_recv()
        if same:
            sends.append((ref, name))

    with scope("pack"):
        for copy in moving[:4]:
            copy.wait()
        size = stage.shape[2] // heads
        for i in range(heads):
            cols = slice(i * size, (i + 1) * size)
            k_pack[i] = jnp.concatenate([stage[0, :, cols], stage[1, :, cols]], axis=1)
            q_pack[i] = jnp.concatenate([stage[2, :, cols], stage[3, :, cols]], axis=1)
        for copy in moving[4:5]:
            copy.wait()
        value_size = v_all.shape[2]
        k_all[s] = k_pack[h]
        q_all[h] = q_pack[h]
        v_all[s] = value_stage[:, pl.ds(pl.multiple_of(h * value_size, value_size), value_size)]

    with scope("barrier"):
        pl.semaphore_wait(barrier, len(peers))

    targets = [other * G + (j + e) % G for e in range(G)]
    targets += [half * G + (j + e) % G for e in range(1, G)]
    for at in targets:
        send(k_pack.at[at % heads], k_all.at[s], "k", at, t)
    for d in range(1, heads):
        i = (h + d) % heads
        send(q_pack.at[i], q_all.at[h], "q", first + i, t)
    for at in targets:
        start = pl.multiple_of((at % heads) * value_size, value_size)
        send(value_stage.at[:, pl.ds(start, value_size)], v_all.at[s], "v", at, t)

    def out_at(zz, xx):
        return outw.at[zz * X + xx]

    rows_chunk = down_weight.shape[0] // C

    def down_at(k):
        return lambda zz, xx: downw.at[zz * X + xx, pl.ds(k * rows_chunk, rows_chunk)]

    def own_z(name, ref):
        for d in range(1, Zh):
            send(ref(zl, x), ref(zl, x), (name, "z", d), z_at(d), t)

    def own_x(name, ref):
        for d in range(1, X):
            send(ref(zl, x), ref(zl, x), (name, "x", d), x_at(d), t)

    def forward_x(name, ref):
        for d in range(1, Zh):
            block = ref(zl_from(d), x)
            arrive(block, (name, "z", d))
            for dx in range(1, X):
                send(block, block, (name, "zx", d, dx), x_at(dx), t)

    def forward_z(name, ref):
        for d in range(1, X):
            block = ref(zl, x_from(d))
            arrive(block, (name, "x", d))
            for dz in range(1, Zh):
                send(block, block, (name, "xz", d, dz), z_at(dz), t)

    def rest_zx(name, ref):
        for d in range(1, X):
            arrive(ref(zl, x_from(d)), (name, "x", d))
        for d in range(1, Zh):
            for dx in range(1, X):
                arrive(ref(zl_from(d), x_from(dx)), (name, "zx", d, dx))

    def rest_xz(name, ref):
        for d in range(1, Zh):
            arrive(ref(zl_from(d), x), (name, "z", d))
        for d in range(1, X):
            for dz in range(1, Zh):
                arrive(ref(zl_from(dz), x_from(d)), (name, "xz", d, dz))

    z_first = list(range(C - X_FIRST)) if C > X_FIRST else list(range(C))
    x_first = [k for k in range(C) if k not in z_first]

    def down(k):
        return "down%d" % k, down_at(k)

    for copy in moving[5:7]:
        copy.wait()
    own_z("out", out_at)
    own_x("out", out_at)
    for e, sp_at in enumerate((s, mate)):
        side = half if e == 0 else other
        for d in range(2):
            cc = c if d == 0 else 1 - c
            start = pl.multiple_of((side * 2 + cc) * quarter, quarter)
            src = residual.at[:, pl.ds(start, quarter)]
            if e or d:
                send(src, res.at[t], "res", sp_at, t_of(half, cc))
            else:
                k = slot("res")
                k_own = slot("res0")

                @pl.when(y == half)
                def _():
                    pltpu.make_async_copy(src, res.at[t], recv_sem.at[k]).start()

                @pl.when(y != half)
                def _():
                    pltpu.make_async_remote_copy(
                        src_ref=src, dst_ref=res.at[t], send_sem=send_sem.at[k_own],
                        recv_sem=recv_sem.at[k], device_id=device(s, t_of(half, cc)),
                        device_id_type=pl.DeviceIdType.MESH,
                    ).start()
    for k in x_first:
        own_x(*down(k))

    with scope("wait_k"):
        arrive(q_all.at[pl.ds(0, heads - 1)], "q")
        arrive(k_all.at[pl.ds(0, sp - 1)], "k")
    with scope("wait_v"):
        arrive(v_all.at[pl.ds(0, sp - 1)], "v")

    pair = q_all.shape[2]
    head_size = pair // 2
    scale = head_size ** (-0.5)
    block_count = max(1, (sp * tokens) // 1024)
    block_sources = sp // block_count
    block_keys = block_sources * tokens
    lanes = lax.broadcasted_iota(jnp.int32, (1, pair), 1) // head_size

    def maps(q):
        stacked = jnp.concatenate(
            [jnp.where(lanes == i, q, jnp.zeros_like(q)) for i in range(2)], axis=0
        )

        def block(b, state):
            rows = pl.ds(b * block_sources, block_sources)
            scores = lax.dot_general(
                stacked, k_all[rows].reshape(block_keys, pair), ROWS_ROWS,
                preferred_element_type=f32,
            )
            newest = jnp.max(scores, axis=1, keepdims=True)
            if state is not None:
                newest = jnp.maximum(newest, state[0])
            shifted = jnp.exp((scores - newest) * scale)
            totals = jnp.sum(shifted, axis=1, keepdims=True)
            product = jnp.dot(
                shifted.astype(bf16), v_all[rows].reshape(block_keys, value_size),
                preferred_element_type=f32,
            )
            if state is not None:
                factor = jnp.exp((state[0] - newest) * scale)
                totals = totals + state[1] * factor
                product = product + state[2] * factor
            return newest, totals, product

        if block_count == 1:
            state = block(0, None)
        else:
            state = lax.fori_loop(
                0,
                block_count,
                block,
                (
                    jnp.full((2 * tokens, 1), -jnp.inf, f32),
                    jnp.zeros((2 * tokens, 1), f32),
                    jnp.zeros((2 * tokens, value_size), f32),
                ),
            )
        return state[2] / state[1]

    head_cols = pl.ds(pl.multiple_of(h * value_size, value_size), value_size)
    with scope("attention"):
        for d in (*range(1, heads), 0):
            i = (h + d) % heads
            both = maps(q_all[i])
            difference = both[:tokens] - lam[h] * both[tokens:]
            scaled = difference * lax.rsqrt(
                jnp.mean(difference * difference, axis=1, keepdims=True) + epsilon
            )
            att_out[d] = (scaled * head_gain[...]).astype(bf16)
            there = att.at[half, :, head_cols]
            send(att_out.at[d], there, "att_other", other * G + (first + i) % G, t)
            if d:
                send(att_out.at[d], there, "att_own", first + i, t)
            else:
                att[half, :, head_cols] = att_out[d]

    with scope("fwd_out"):
        forward_x("out", out_at)
    for k in z_first[:2]:
        own_z(*down(k))
    with scope("wait_out"):
        rest_zx("out", out_at)
    with scope("wait_att"):
        arrive(v_all.at[pl.ds(0, heads - 1)], "att_own")
        arrive(v_all.at[pl.ds(0, heads)], "att_other")

    core_mate = t_of(y, 1 - c)
    width_out = att.shape[2]
    many = G // 2

    with scope("outproj"):
        rows_in = att[...].reshape(2 * tokens, width_out)

        def project(side):
            weight = outw[pl.ds(side * many, many)].reshape(quarter, width_out)
            return lax.dot_general(rows_in, weight, ROWS_ROWS, preferred_element_type=f32)

        core_out[0] = project(1 - c).astype(bf16)
        send(core_out.at[0], core_in.at[0], "p1c", s, core_mate)
        own_sum[...] = project(c)
        for k in z_first:
            own_x(*down(k))
    with scope("wait_p1c"):
        arrive(core_in.at[0], "p1c")

    def slot_rows(yy):
        return pl.ds(pl.multiple_of(yy * tokens, tokens), tokens)

    with scope("sum_c"):
        for d in range(1, Y):
            yy = (y + d) % Y
            rows = slot_rows(yy)
            y_out[d - 1] = (own_sum[rows] + core_in[0, rows].astype(f32)).astype(bf16)
            send(y_out.at[d - 1], y_in.at[d - 1], ("p1y", d), s, t_of(yy, c))
    with scope("wait_res"):
        wait(res, "res").wait_recv()
    with scope("wait_p1y"):
        for d in range(1, Y):
            arrive(y_in.at[d - 1], ("p1y", d))
    q_own = half * 2 + c
    q_mate = other * 2 + c

    def block_at(yy, q, k=None):
        cols = pl.ds(pl.multiple_of(q * quarter, quarter), quarter)
        size = tokens // PIECES
        rows = pl.ds(0, tokens) if k is None else pl.ds(k * size, size)
        return full.at[yy, rows, cols]

    with scope("sum_y"):
        rows = slot_rows(y)
        total = own_sum[rows] + core_in[0, rows].astype(f32)
        for d in range(1, Y):
            total = total + y_in[d - 1].astype(f32)
        total = total + res[...].reshape(tokens, quarter).astype(f32)
        full[y, :, pl.ds(pl.multiple_of(q_own * quarter, quarter), quarter)] = total.astype(bf16)
        for k in range(PIECES):
            block = block_at(y, q_own, k)
            send(block, block, ("az", k), mate, t)
        for d in range(1, Y):
            block = block_at(y, q_own)
            send(block, block, ("ay", d), s, t_of((y + d) % Y, c))
        block = block_at(y, q_own)
        send(block, block, "ad", s, core_mate)
        for k in z_first[2:] + x_first:
            own_z(*down(k))

    with scope("wait_ay"):
        for d in range(1, Y):
            block = block_at((y - d + Y) % Y, q_own)
            arrive(block, ("ay", d))
            send(block, block, "ad", s, core_mate)
    with scope("wait_az"):
        for k in range(PIECES):
            block = block_at(y, q_mate, k)
            arrive(block, ("az", k))
            for d in range(1, Y):
                send(block, block, ("ayz", d, k), s, t_of((y + d) % Y, c))
            send(block, block, "ad", s, core_mate)
    with scope("fwd_down_a"):
        for k in z_first[:2]:
            forward_x(*down(k))
    with scope("wait_ayz"):
        for k in range(PIECES):
            for d in range(1, Y):
                block = block_at((y - d + Y) % Y, q_mate, k)
                arrive(block, ("ayz", d, k))
                send(block, block, "ad", s, core_mate)
    with scope("wait_ad"):
        arrive(full.at[0], "ad")

    with scope("norm"):
        step = min(32, tokens)
        for yy in range(2):
            for at in range(0, tokens, step):
                stream = full[yy, at : at + step].astype(f32)
                scaled = stream * lax.rsqrt(
                    jnp.mean(stream * stream, axis=1, keepdims=True) + epsilon
                )
                normed[yy * tokens + at : yy * tokens + at + step] = (
                    scaled * norm_gain[...]
                ).astype(bf16)

    for copy in moving[7:]:
        copy.wait()
    width = hidden.shape[1]
    spans = [(at, min(512, width - at)) for at in range(0, width, 512)]
    with scope("gateup"):
        rows_in = normed[...]
        for at, n in spans:
            gate_part = jnp.dot(rows_in, gate[:, at : at + n], preferred_element_type=f32)
            up_part = jnp.dot(rows_in, up[:, at : at + n], preferred_element_type=f32)
            hidden[:, at : at + n] = (
                gate_part / (1.0 + jnp.exp(-gate_part)) * up_part
            ).astype(bf16)
    with scope("fwd_down_b"):
        for k in z_first[2:]:
            forward_x(*down(k))
        for k in x_first:
            forward_z(*down(k))
    with scope("wait_down"):
        for k in z_first:
            rest_zx(*down(k))
        for k in x_first:
            rest_xz(*down(k))

    with scope("downmm"):
        def lower(side):
            weight = downw[pl.ds(side * many, many)].reshape(quarter, width)
            return lax.dot_general(hidden[...], weight, ROWS_ROWS, preferred_element_type=f32)

        core_out[1] = lower(1 - c).astype(bf16)
        send(core_out.at[1], core_in.at[1], "p2c", s, core_mate)
        own_sum[...] = lower(c)
    with scope("wait_p2c"):
        arrive(core_in.at[1], "p2c")
    place = q_own * Y + y
    with scope("sum2"):
        owner_out[...] = (
            (own_sum[...] + core_in[1].astype(f32)).astype(bf16).reshape(2, T, piece, quarter)
        )
        for d in range(T):
            at = (t + d) % T
            send(owner_out.at[other, at], owner_in.at[place], "p2o", mate, at)
        for d in range(1, T):
            at = (t + d) % T
            send(owner_out.at[half, at], owner_in.at[place], "p2o", s, at)
        owner_in[place] = owner_out[half, t]
    with scope("wait_p2o"):
        arrive(owner_in.at[pl.ds(0, 4 * Y - 1)], "p2o")
    with scope("final"):
        mine = pl.ds(pl.multiple_of(t * piece, piece), piece)
        for q in range(4):
            cols = slice(q * quarter, (q + 1) * quarter)
            total = owner_in[q * Y].astype(f32)
            for i in range(1, Y):
                total = total + owner_in[q * Y + i].astype(f32)
            result[:, cols] = (full[half, mine, cols].astype(f32) + total).astype(bf16)
    with scope("wait_send"):
        for ref, name in sends:
            wait(ref, name).wait_send()
        wait(res.at[pl.ds(0, 3)], "res").wait_send()

        @pl.when(y != half)
        def _():
            wait(res.at[0], "res0").wait_send()


def local(Z, X, T, *arrays):
    (residual, q_one, k_one, q_two, k_two, values, lam, head_gain, out_weight, norm_gain,
     gate_weight, up_weight, down_weight) = arrays
    sp = Z * X
    G = sp // 2
    bf16 = jnp.bfloat16
    heads = lam.shape[0]
    tokens, kw = k_one.shape
    vw = values.shape[1]
    pair = 2 * (kw // heads)
    vd = vw // heads
    piece, model = residual.shape
    quarter = model // 4
    width = gate_weight.shape[1]
    rows_down = down_weight.shape[0]
    C = max(1, min(CHUNKS, rows_down // 16))
    Y = T // 2
    vmem = pl.BlockSpec(memory_space=pltpu.VMEM)
    anywhere = pl.BlockSpec(memory_space=pl.ANY)
    smem = pl.BlockSpec(memory_space=pltpu.SMEM)
    Zh = Z // 2
    semaphores = 24 + (1 + C) * (Zh - 1 + X - 1 + (Zh - 1) * (X - 1))
    return pl.pallas_call(
        functools.partial(kernel, Z, X, T, C, heads),
        out_shape=jax.ShapeDtypeStruct((piece, model), bf16),
        in_specs=[
            anywhere, anywhere, anywhere, anywhere, anywhere, anywhere, smem, vmem, anywhere, vmem,
            anywhere, anywhere, anywhere,
        ],
        out_specs=vmem,
        scratch_shapes=[
            pltpu.VMEM((4, tokens, kw), bf16),
            pltpu.VMEM((tokens, vw), bf16),
            pltpu.VMEM((heads, tokens, pair), bf16),
            pltpu.VMEM((heads, tokens, pair), bf16),
            pltpu.VMEM((heads, tokens, pair), bf16),
            pltpu.VMEM((sp, tokens, pair), bf16),
            pltpu.VMEM((sp, tokens, vd), bf16),
            pltpu.VMEM((G, out_weight.shape[0], vw), bf16),
            pltpu.VMEM((G, rows_down, width), bf16),
            pltpu.VMEM(gate_weight.shape, bf16),
            pltpu.VMEM(up_weight.shape, bf16),
            pltpu.VMEM((heads, tokens, vd), bf16),
            pltpu.VMEM((2, tokens, vw), bf16),
            pltpu.VMEM((T, piece, quarter), bf16),
            pltpu.VMEM((2, 2 * tokens, quarter), bf16),
            pltpu.VMEM((2, 2 * tokens, quarter), bf16),
            pltpu.VMEM((Y - 1, tokens, quarter), bf16),
            pltpu.VMEM((Y - 1, tokens, quarter), bf16),
            pltpu.VMEM((2 * tokens, quarter), jnp.float32),
            pltpu.VMEM((2, tokens, model), bf16),
            pltpu.VMEM((2 * tokens, model), bf16),
            pltpu.VMEM((2 * tokens, width), bf16),
            pltpu.VMEM((2, T, piece, quarter), bf16),
            pltpu.VMEM((4 * Y, piece, quarter), bf16),
            pltpu.SemaphoreType.DMA((9,)),
            pltpu.SemaphoreType.DMA((semaphores,)),
            pltpu.SemaphoreType.DMA((semaphores,)),
        ],
        compiler_params=pltpu.CompilerParams(
            collective_id=0, has_side_effects=True, vmem_limit_bytes=60 * 1024 * 1024
        ),
    )(
        residual, q_one, k_one, q_two, k_two, values, lam, head_gain.reshape(1, -1), out_weight,
        norm_gain.reshape(1, -1), gate_weight, up_weight, down_weight,
    )


def solution(mesh):
    Z, X = split_sp(mesh.shape["sp"])
    return jax.shard_map(
        functools.partial(local, Z, X, mesh.shape["tp"]),
        mesh=mesh,
        in_specs=(
            P(("sp", "tp"), None),
            P("sp", "tp"),
            P("sp", "tp"),
            P("sp", "tp"),
            P("sp", "tp"),
            P("sp", "tp"),
            P("tp"),
            P(),
            P("sp", "tp"),
            P(),
            P(None, "tp"),
            P(None, "tp"),
            P("sp", "tp"),
        ),
        out_specs=P(("sp", "tp"), None),
        check_vma=False,
    )
```

```python
import functools

import jax
import jax.numpy as jnp
from jax import lax
from jax.experimental import pallas as pl
from jax.experimental.pallas import tpu as pltpu
from jax.sharding import PartitionSpec as P

epsilon = 1e-06
ROWS_ROWS = (((1,), (1,)), ((), ()))
CHUNKS = 8
X_FIRST = 3
OUT_CHUNKS = 4
S0 = 1
S1 = 1
S2 = 2
PIECES = 4


def split_sp(size):
    inner = 1
    while (2 * inner) * (2 * inner) <= size:
        inner *= 2
    return size // inner, inner


def kernel(
    Z,
    X,
    T,
    C,
    OC,
    heads,
    residual,
    q_one,
    k_one,
    q_two,
    k_two,
    values,
    lam,
    head_gain,
    out_weight,
    norm_gain,
    gate_weight,
    up_weight,
    down_weight,
    result,
    stage,
    value_stage,
    q_pack,
    k_pack,
    q_all,
    k_all,
    v_all,
    outw,
    downw,
    gate,
    up,
    att_out,
    att,
    res,
    core_out,
    core_in,
    prod,
    lower_out,
    lower_in,
    y_out,
    y_in,
    own_sum,
    full,
    normed,
    hidden,
    owner_out,
    owner_in,
    local_sem,
    send_sem,
    recv_sem,
):
    f32, bf16 = jnp.float32, jnp.bfloat16
    scope = jax.named_scope
    s = lax.axis_index("sp")
    t = lax.axis_index("tp")
    z, x = s // X, s % X
    sp = Z * X
    Zh = Z // 2
    G = Zh * X
    half = z // Zh
    other = 1 - half
    zl = z % Zh
    j = zl * X + x
    mate = other * G + j
    Y = T // 2
    y, c = t // 2, t % 2
    tokens = q_one.shape[0]
    piece = tokens // T
    down_rows = down_weight.shape[0]
    h = s % heads
    first = s - h
    quarter = full.shape[2] // 4

    def z_at(d):
        return (half * Zh + (zl + d) % Zh) * X + x

    def zl_from(d):
        return (zl - d + Zh) % Zh

    def x_at(d):
        return z * X + (x + d) % X

    def x_from(d):
        return (x - d + X) % X

    def t_of(yy, cc):
        return yy * 2 + cc

    def device(sp_at, tp_at):
        return {"sp": sp_at, "tp": tp_at}

    moves = [
        (k_one, stage.at[0]),
        (k_two, stage.at[1]),
        (q_one, stage.at[2]),
        (q_two, stage.at[3]),
        (values, value_stage),
        (out_weight, outw.at[j]),
        (down_weight, downw.at[pl.ds(pl.multiple_of(j * down_rows, down_rows), down_rows)]),
        (gate_weight, gate),
        (up_weight, up),
    ]
    moving = [
        pltpu.make_async_copy(src, dst, local_sem.at[i]) for i, (src, dst) in enumerate(moves)
    ]
    for copy in moving:
        copy.start()

    barrier = pltpu.get_barrier_semaphore()
    peers = [((s + d) % sp, t) for d in range(1, sp)]
    peers += [(s, (t + d) % T) for d in range(1, T)]
    peers += [(mate, (t + d) % T) for d in range(1, T)]
    for sp_at, tp_at in peers:
        pl.semaphore_signal(
            barrier, inc=1, device_id=device(sp_at, tp_at), device_id_type=pl.DeviceIdType.MESH
        )

    names = {}
    send_names = {}
    sends = []

    def slot(name):
        return names.setdefault(name, len(names))

    def send_slot(name):
        return send_names.setdefault(name, len(send_names))

    def send(src, dst, name, sp_at, tp_at, group=None):
        pltpu.make_async_remote_copy(
            src_ref=src, dst_ref=dst, send_sem=send_sem.at[send_slot(group or name)],
            recv_sem=recv_sem.at[slot(name)], device_id=device(sp_at, tp_at),
            device_id_type=pl.DeviceIdType.MESH,
        ).start()

    def wait(ref, send_at, recv_at):
        return pltpu.make_async_remote_copy(
            src_ref=ref, dst_ref=ref, send_sem=send_sem.at[send_at], recv_sem=recv_sem.at[recv_at],
            device_id=device(s, t), device_id_type=pl.DeviceIdType.MESH,
        )

    def arrive(ref, name, same=True):
        wait(ref, 0, slot(name)).wait_recv()
        if same:
            sends.append((ref, name))

    def sent(ref, name):
        wait(ref, send_slot(name), 0).wait_send()

    with scope("pack"):
        for copy in moving[:4]:
            copy.wait()
        size = stage.shape[2] // heads
        for i in range(heads):
            cols = slice(i * size, (i + 1) * size)
            k_pack[i] = jnp.concatenate([stage[0, :, cols], stage[1, :, cols]], axis=1)
            q_pack[i] = jnp.concatenate([stage[2, :, cols], stage[3, :, cols]], axis=1)
        for copy in moving[4:5]:
            copy.wait()
        value_size = v_all.shape[2]
        k_all[s] = k_pack[h]
        q_all[h] = q_pack[h]
        v_all[s] = value_stage[:, pl.ds(pl.multiple_of(h * value_size, value_size), value_size)]

    with scope("barrier"):
        pl.semaphore_wait(barrier, len(peers))

    targets = [other * G + (j + e) % G for e in range(G)]
    targets += [half * G + (j + e) % G for e in range(1, G)]
    for at in targets:
        send(k_pack.at[at % heads], k_all.at[s], "k", at, t)
    for d in range(1, heads):
        i = (h + d) % heads
        send(q_pack.at[i], q_all.at[h], "q", first + i, t)
    for at in targets:
        start = pl.multiple_of((at % heads) * value_size, value_size)
        send(value_stage.at[:, pl.ds(start, value_size)], v_all.at[s], "v", at, t)

    def rows_of(ref, count, k):
        size = ref.shape[1] // count
        return lambda zz, xx: ref.at[zz * X + xx, pl.ds(k * size, size)]

    def down_part(k):
        size = down_rows // C

        def at(zz, xx):
            start = pl.multiple_of((zz * X + xx) * down_rows + k * size, size)
            return downw.at[pl.ds(start, size)]

        return at

    def own_z(name, ref, group, last):
        for d in range(1, Zh):
            to = group + "_z" if last else (name, "z", d)
            send(ref(zl, x), ref(zl, x), to, z_at(d), t, group)

    def own_x(name, ref, group, last):
        for d in range(1, X):
            to = group + "_x" if last else (name, "x", d)
            send(ref(zl, x), ref(zl, x), to, x_at(d), t, group)

    def forward_x(name, ref, group):
        for d in range(1, Zh):
            block = ref(zl_from(d), x)
            arrive(block, (name, "z", d), False)
            for dx in range(1, X):
                send(block, block, group + "_rest", x_at(dx), t, group)

    def forward_z(name, ref, group):
        for d in range(1, X):
            block = ref(zl, x_from(d))
            arrive(block, (name, "x", d), False)
            for dz in range(1, Zh):
                send(block, block, group + "_rest", z_at(dz), t, group)

    def down(k):
        return "down%d" % k, down_part(k), "down"

    def out(k):
        return "out%d" % k, rows_of(outw, OC, k), "out"

    z_first = list(range(C - X_FIRST)) if C > X_FIRST else list(range(C))
    x_first = [k for k in range(C) if k not in z_first]

    nx = len(x_first)
    for copy in moving[5:7]:
        copy.wait()
    for k in range(OC):
        own_z(*out(k), False)
        own_x(*out(k), True)
    for e, sp_at in enumerate((s, mate)):
        side = half if e == 0 else other
        for d in range(2):
            cc = c if d == 0 else 1 - c
            start = pl.multiple_of((side * 2 + cc) * quarter, quarter)
            src = residual.at[:, pl.ds(start, quarter)]
            if e or d:
                send(src, res.at[t], "res", sp_at, t_of(half, cc))
            else:
                k = slot("res")
                k_own = send_slot("res0")

                @pl.when(y == half)
                def _():
                    pltpu.make_async_copy(src, res.at[t], recv_sem.at[k]).start()

                @pl.when(y != half)
                def _():
                    pltpu.make_async_remote_copy(
                        src_ref=src, dst_ref=res.at[t], send_sem=send_sem.at[k_own],
                        recv_sem=recv_sem.at[k], device_id=device(s, t_of(half, cc)),
                        device_id_type=pl.DeviceIdType.MESH,
                    ).start()
    for k in x_first[:S0]:
        own_x(*down(k), False)

    with scope("wait_k"):
        arrive(q_all.at[pl.ds(0, heads - 1)], "q")
        arrive(k_all.at[pl.ds(0, sp - 1)], "k")
    with scope("wait_v"):
        arrive(v_all.at[pl.ds(0, sp - 1)], "v")

    pair = q_all.shape[2]
    head_size = pair // 2
    scale = head_size ** (-0.5)
    block_count = max(1, (sp * tokens) // 1024)
    block_sources = sp // block_count
    block_keys = block_sources * tokens
    lanes = lax.broadcasted_iota(jnp.int32, (1, pair), 1) // head_size

    def maps(q):
        stacked = jnp.concatenate(
            [jnp.where(lanes == i, q, jnp.zeros_like(q)) for i in range(2)], axis=0
        )

        def block(b, state):
            rows = pl.ds(b * block_sources, block_sources)
            scores = lax.dot_general(
                stacked, k_all[rows].reshape(block_keys, pair), ROWS_ROWS,
                preferred_element_type=f32,
            )
            newest = jnp.max(scores, axis=1, keepdims=True)
            if state is not None:
                newest = jnp.maximum(newest, state[0])
            shifted = jnp.exp((scores - newest) * scale)
            totals = jnp.sum(shifted, axis=1, keepdims=True)
            product = jnp.dot(
                shifted.astype(bf16), v_all[rows].reshape(block_keys, value_size),
                preferred_element_type=f32,
            )
            if state is not None:
                factor = jnp.exp((state[0] - newest) * scale)
                totals = totals + state[1] * factor
                product = product + state[2] * factor
            return newest, totals, product

        if block_count == 1:
            state = block(0, None)
        else:
            state = lax.fori_loop(
                0,
                block_count,
                block,
                (
                    jnp.full((2 * tokens, 1), -jnp.inf, f32),
                    jnp.zeros((2 * tokens, 1), f32),
                    jnp.zeros((2 * tokens, value_size), f32),
                ),
            )
        return state[2] / state[1]

    head_cols = pl.ds(pl.multiple_of(h * value_size, value_size), value_size)
    with scope("attention"):
        for turn, d in enumerate((*range(1, heads), 0)):
            i = (h + d) % heads
            both = maps(q_all[i])
            difference = both[:tokens] - lam[h] * both[tokens:]
            scaled = difference * lax.rsqrt(
                jnp.mean(difference * difference, axis=1, keepdims=True) + epsilon
            )
            att_out[d] = (scaled * head_gain[...]).astype(bf16)
            there = att.at[half, :, head_cols]
            send(att_out.at[d], there, "att_other", other * G + (first + i) % G, t)
            if d:
                send(att_out.at[d], there, "att_own", first + i, t)
            else:
                att[half, :, head_cols] = att_out[d]
            if 0 < turn <= OC:
                forward_x(*out(turn - 1))

    with scope("fwd_out"):
        for k in range(heads - 1, OC):
            forward_x(*out(k))
        for k in x_first[S0 : S0 + S1]:
            own_x(*down(k), False)
        for k in z_first[:S2]:
            own_z(*down(k), False)
    with scope("wait_att_own"):
        arrive(v_all.at[pl.ds(0, heads - 1)], "att_own")
    with scope("wait_att"):
        arrive(v_all.at[pl.ds(0, heads)], "att_other")
    with scope("wait_out"):
        arrive(outw.at[pl.ds(0, X - 1)], "out_x", False)
        arrive(outw.at[pl.ds(0, (X - 1) * (Zh - 1))], "out_rest", False)
    for k in z_first[S2:]:
        own_z(*down(k), False)
    for k in x_first[S0 + S1 :]:
        own_x(*down(k), False)

    core_mate = t_of(y, 1 - c)
    width_out = att.shape[2]
    many = G // 2

    with scope("outproj"):
        rows_in = att[...].reshape(2 * tokens, width_out)

        def project(side):
            weight = outw[pl.ds(side * many, many)].reshape(quarter, width_out)
            return lax.dot_general(rows_in, weight, ROWS_ROWS, preferred_element_type=f32)

        core_out[0] = project(1 - c).astype(bf16)
        send(core_out.at[0], core_in.at[0], "p1c", s, core_mate)
        own_sum[...] = project(c)
        for k in z_first:
            own_x(*down(k), True)
    with scope("wait_p1c"):
        arrive(core_in.at[0], "p1c")

    def slot_rows(yy):
        return pl.ds(pl.multiple_of(yy * tokens, tokens), tokens)

    part = tokens // PIECES

    def slot_rows(yy, k):
        return pl.ds(pl.multiple_of(yy * tokens + k * part, part), part)

    with scope("sum_c"):
        for k in range(PIECES):
            for d in range(1, Y):
                yy = (y + d) % Y
                rows = slot_rows(yy, k)
                block = y_out.at[d - 1, pl.ds(k * part, part)]
                y_out[d - 1, k * part : (k + 1) * part] = (
                    own_sum[rows] + core_in[0, rows].astype(f32)
                ).astype(bf16)
                there = y_in.at[d - 1, pl.ds(k * part, part)]
                send(block, there, ("p1y", d, k), s, t_of(yy, c), "after")
    with scope("wait_res"):
        arrive(res, "res", False)
    q_own = half * 2 + c
    q_mate = other * 2 + c

    def block_at(yy, q, k=None):
        cols = pl.ds(pl.multiple_of(q * quarter, quarter), quarter)
        rows = pl.ds(0, tokens) if k is None else pl.ds(k * part, part)
        return full.at[yy, rows, cols]

    with scope("sum_y"):
        residual_rows = res[...].reshape(tokens, quarter)
        own_cols = pl.ds(pl.multiple_of(q_own * quarter, quarter), quarter)
        for k in range(PIECES):
            rows = slot_rows(y, k)
            here = slice(k * part, (k + 1) * part)
            total = own_sum[rows] + core_in[0, rows].astype(f32)
            for d in range(1, Y):
                arrive(y_in.at[d - 1, pl.ds(k * part, part)], ("p1y", d, k), False)
                total = total + y_in[d - 1, here].astype(f32)
            total = total + residual_rows[here].astype(f32)
            full[y, here, own_cols] = total.astype(bf16)
            block = block_at(y, q_own, k)
            send(block, block, ("az", k), mate, t, "after")
            for d in range(1, Y):
                send(block, block, ("ay", d), s, t_of((y + d) % Y, c), "after")
        block = block_at(y, q_own)
        send(block, block, "ad", s, core_mate)
    with scope("bulk_a"):
        for k in z_first[:3]:
            forward_x(*down(k))
        for k in x_first[: nx - 1]:
            own_z(*down(k), True)
            forward_z(*down(k))

    with scope("wait_ay"):
        for d in range(1, Y):
            block = block_at((y - d + Y) % Y, q_own)
            arrive(block, ("ay", d), False)
            send(block, block, "ad", s, core_mate)
    with scope("wait_az"):
        for k in range(PIECES):
            block = block_at(y, q_mate, k)
            arrive(block, ("az", k), False)
            for d in range(1, Y):
                send(block, block, ("ayz", d, k), s, t_of((y + d) % Y, c), "after")
            send(block, block, "ad", s, core_mate)
    with scope("bulk_b"):
        for k in z_first[3:]:
            forward_x(*down(k))
        for k in x_first[nx - 1 :]:
            own_z(*down(k), True)
            forward_z(*down(k))
    with scope("wait_ayz"):
        for k in range(PIECES):
            for d in range(1, Y):
                block = block_at((y - d + Y) % Y, q_mate, k)
                arrive(block, ("ayz", d, k), False)
                send(block, block, "ad", s, core_mate)
    with scope("wait_ad"):
        arrive(full.at[0], "ad")

    with scope("norm"):
        step = min(32, tokens)
        for yy in range(2):
            for at in range(0, tokens, step):
                stream = full[yy, at : at + step].astype(f32)
                scaled = stream * lax.rsqrt(
                    jnp.mean(stream * stream, axis=1, keepdims=True) + epsilon
                )
                normed[yy * tokens + at : yy * tokens + at + step] = (
                    scaled * norm_gain[...]
                ).astype(bf16)

    for copy in moving[7:]:
        copy.wait()
    width = hidden.shape[1]
    spans = [(at, min(512, width - at)) for at in range(0, width, 512)]
    with scope("gateup"):
        rows_in = normed[...]
        for at, n in spans:
            gate_part = jnp.dot(rows_in, gate[:, at : at + n], preferred_element_type=f32)
            up_part = jnp.dot(rows_in, up[:, at : at + n], preferred_element_type=f32)
            hidden[:, at : at + n] = (
                gate_part / (1.0 + jnp.exp(-gate_part)) * up_part
            ).astype(bf16)
    place = q_own * Y + y
    unit = prod.shape[2]
    half_unit = unit // 2
    size = down_rows // C
    staged = G == 4 and X == 2
    if staged:
        order = [j, zl * X + 1 - x, (1 - zl) * X + x, (1 - zl) * X + 1 - x]
    else:
        order = list(range(4))

    def lower(i):
        weight = downw[pl.ds(pl.multiple_of(order[i] * unit, unit), unit)]
        prod[i] = lax.dot_general(hidden[...], weight, ROWS_ROWS, preferred_element_type=f32)
        cols = pl.ds(pl.multiple_of((1 - c) * half_unit, half_unit), half_unit)
        lower_out[i] = prod[i, :, cols].astype(bf16)

    def pass_on(lo, n, name):
        units = pl.ds(lo, n)
        send(lower_out.at[units], lower_in.at[units], name, s, core_mate)

    def to_owners(lo, n, name, core_name):
        units = pl.ds(lo, n)
        arrive(lower_in.at[units], core_name)
        cols = pl.ds(pl.multiple_of(c * half_unit, half_unit), half_unit)
        for i in range(lo, lo + n):
            total = prod[i, :, cols] + lower_in[i].astype(f32)
            owner_out[:, :, i] = total.astype(bf16).reshape(2, T, piece, half_unit)
        for d in range(T):
            at = (t + d) % T
            send(owner_out.at[other, at, units], owner_in.at[place, units], name, mate, at)
        for d in range(1, T):
            at = (t + d) % T
            send(owner_out.at[half, at, units], owner_in.at[place, units], name, s, at)
        owner_in[place, units] = owner_out[half, t, units]

    def wait_x():
        if z_first:
            arrive(downw.at[pl.ds(0, len(z_first) * (X - 1) * size)], "down_x", False)

    def wait_z():
        if x_first:
            arrive(downw.at[pl.ds(0, nx * (Zh - 1) * size)], "down_z", False)

    def wait_rest():
        arrive(downw.at[pl.ds(0, (X - 1) * (Zh - 1) * down_rows)], "down_rest", False)

    if not staged:
        wait_x()
        wait_z()
        wait_rest()
    with scope("down_a"):
        lower(0)
        if staged:
            with scope("wait_x"):
                wait_x()
        lower(1)
        if staged:
            with scope("wait_z"):
                wait_z()
        lower(2)
        pass_on(0, 3, "p2c")
    with scope("owners_a"):
        to_owners(0, 3, "p2o", "p2c")
    if staged:
        with scope("wait_rest"):
            wait_rest()
    with scope("down_b"):
        lower(3)
        pass_on(3, 1, "p3c")
        to_owners(3, 1, "p3o", "p3c")
    mine = pl.ds(pl.multiple_of(t * piece, piece), piece)

    def finish(lo, n, name):
        arrive(owner_in.at[pl.ds(0, 4 * Y - 1), pl.ds(lo, n)], name)
        for q in range(4):
            for i in range(lo, lo + n):
                start = (q // 2) * 4 * unit + order[i] * unit + (q % 2) * half_unit
                cols = pl.ds(pl.multiple_of(start, half_unit), half_unit)
                total = owner_in[q * Y, i].astype(f32)
                for k in range(1, Y):
                    total = total + owner_in[q * Y + k, i].astype(f32)
                result[:, cols] = (full[half, mine, cols].astype(f32) + total).astype(bf16)

    with scope("wait_p2o"):
        finish(0, 3, "p2o")
    with scope("wait_p3o"):
        finish(3, 1, "p3o")
    with scope("wait_send"):
        for ref, name in sends:
            sent(ref, name)
        sent(outw.at[pl.ds(0, G - 1)], "out")
        sent(downw.at[pl.ds(0, (G - 1) * down_rows)], "down")
        assert 3 * (Y - 1) + 1 == 4
        sent(full.at[0], "after")
        sent(res.at[pl.ds(0, 3)], "res")

        @pl.when(y != half)
        def _():
            sent(res.at[0], "res0")
    assert len(names) <= recv_sem.shape[0] and len(send_names) <= send_sem.shape[0]


def local(Z, X, T, *arrays):
    (residual, q_one, k_one, q_two, k_two, values, lam, head_gain, out_weight, norm_gain,
     gate_weight, up_weight, down_weight) = arrays
    sp = Z * X
    G = sp // 2
    bf16 = jnp.bfloat16
    heads = lam.shape[0]
    tokens, kw = k_one.shape
    vw = values.shape[1]
    pair = 2 * (kw // heads)
    vd = vw // heads
    piece, model = residual.shape
    quarter = model // 4
    width = gate_weight.shape[1]
    rows_down = down_weight.shape[0]
    C = max(1, min(CHUNKS, rows_down // 16))
    OC = max(1, min(OUT_CHUNKS, out_weight.shape[0] // 16))
    Y = T // 2
    vmem = pl.BlockSpec(memory_space=pltpu.VMEM)
    anywhere = pl.BlockSpec(memory_space=pl.ANY)
    smem = pl.BlockSpec(memory_space=pltpu.SMEM)
    Zh = Z // 2
    z_first = C - X_FIRST if C > X_FIRST else C
    received = 20 + 4 * PIECES + (OC + z_first) * (Zh - 1) + (C - z_first) * (X - 1)
    return pl.pallas_call(
        functools.partial(kernel, Z, X, T, C, OC, heads),
        out_shape=jax.ShapeDtypeStruct((piece, model), bf16),
        in_specs=[
            anywhere, anywhere, anywhere, anywhere, anywhere, anywhere, smem, vmem, anywhere, vmem,
            anywhere, anywhere, anywhere,
        ],
        out_specs=vmem,
        scratch_shapes=[
            pltpu.VMEM((4, tokens, kw), bf16),
            pltpu.VMEM((tokens, vw), bf16),
            pltpu.VMEM((heads, tokens, pair), bf16),
            pltpu.VMEM((heads, tokens, pair), bf16),
            pltpu.VMEM((heads, tokens, pair), bf16),
            pltpu.VMEM((sp, tokens, pair), bf16),
            pltpu.VMEM((sp, tokens, vd), bf16),
            pltpu.VMEM((G, out_weight.shape[0], vw), bf16),
            pltpu.VMEM((G * rows_down, width), bf16),
            pltpu.VMEM(gate_weight.shape, bf16),
            pltpu.VMEM(up_weight.shape, bf16),
            pltpu.VMEM((heads, tokens, vd), bf16),
            pltpu.VMEM((2, tokens, vw), bf16),
            pltpu.VMEM((T, piece, quarter), bf16),
            pltpu.VMEM((1, 2 * tokens, quarter), bf16),
            pltpu.VMEM((1, 2 * tokens, quarter), bf16),
            pltpu.VMEM((4, 2 * tokens, model // 8), jnp.float32),
            pltpu.VMEM((4, 2 * tokens, model // 16), bf16),
            pltpu.VMEM((4, 2 * tokens, model // 16), bf16),
            pltpu.VMEM((Y - 1, tokens, quarter), bf16),
            pltpu.VMEM((Y - 1, tokens, quarter), bf16),
            pltpu.VMEM((2 * tokens, quarter), jnp.float32),
            pltpu.VMEM((2, tokens, model), bf16),
            pltpu.VMEM((2 * tokens, model), bf16),
            pltpu.VMEM((2 * tokens, width), bf16),
            pltpu.VMEM((2, T, 4, piece, model // 16), bf16),
            pltpu.VMEM((4 * Y, 4, piece, model // 16), bf16),
            pltpu.SemaphoreType.DMA((9,)),
            pltpu.SemaphoreType.DMA((16,)),
            pltpu.SemaphoreType.DMA((received,)),
        ],
        compiler_params=pltpu.CompilerParams(
            collective_id=0, has_side_effects=True, vmem_limit_bytes=60 * 1024 * 1024
        ),
    )(
        residual, q_one, k_one, q_two, k_two, values, lam, head_gain.reshape(1, -1), out_weight,
        norm_gain.reshape(1, -1), gate_weight, up_weight, down_weight,
    )


def solution(mesh):
    Z, X = split_sp(mesh.shape["sp"])
    return jax.shard_map(
        functools.partial(local, Z, X, mesh.shape["tp"]),
        mesh=mesh,
        in_specs=(
            P(("sp", "tp"), None),
            P("sp", "tp"),
            P("sp", "tp"),
            P("sp", "tp"),
            P("sp", "tp"),
            P("sp", "tp"),
            P("tp"),
            P(),
            P("sp", "tp"),
            P(),
            P(None, "tp"),
            P(None, "tp"),
            P("sp", "tp"),
        ),
        out_specs=P(("sp", "tp"), None),
        check_vma=False,
    )
```

```python
import functools

import jax
import jax.numpy as jnp
from jax import lax
from jax.experimental import pallas as pl
from jax.experimental.pallas import tpu as pltpu
from jax.sharding import PartitionSpec as P

epsilon = 1e-06
ROWS_ROWS = (((1,), (1,)), ((), ()))
CHUNKS = 8
S3 = 1
X_FIRST = 3
OUT_CHUNKS = 4
S0 = 1
S1 = 1
S2 = 5
OUT_X_FIRST = 0
PIECES = 4


def split_sp(size):
    inner = 1
    while (2 * inner) * (2 * inner) <= size:
        inner *= 2
    return size // inner, inner


def kernel(
    Z,
    X,
    T,
    C,
    OC,
    heads,
    residual,
    q_one,
    k_one,
    q_two,
    k_two,
    values,
    lam,
    head_gain,
    out_weight,
    norm_gain,
    gate_weight,
    up_weight,
    down_weight,
    result,
    stage,
    value_stage,
    q_pack,
    k_pack,
    q_all,
    k_all,
    v_all,
    outw,
    downw,
    gate,
    up,
    head_scale,
    norm_scale,
    rounded_all,
    totals_all,
    att_out,
    att,
    res,
    core_out,
    core_in,
    prod,
    lower_out,
    lower_in,
    y_out,
    y_in,
    own_sum,
    full,
    normed,
    squares,
    inverse,
    gate_sum,
    up_sum,
    hidden,
    owner_out,
    owner_in,
    local_sem,
    send_sem,
    recv_sem,
):
    f32, bf16 = jnp.float32, jnp.bfloat16
    scope = jax.named_scope
    s = lax.axis_index("sp")
    t = lax.axis_index("tp")
    z, x = s // X, s % X
    sp = Z * X
    Zh = Z // 2
    G = Zh * X
    half = z // Zh
    other = 1 - half
    zl = z % Zh
    j = zl * X + x
    mate = other * G + j
    Y = T // 2
    y, c = t // 2, t % 2
    tokens = q_one.shape[0]
    piece = tokens // T
    down_rows = down_weight.shape[0]
    h = s % heads
    first = s - h
    quarter = full.shape[2] // 4

    def z_at(d):
        return (half * Zh + (zl + d) % Zh) * X + x

    def zl_from(d):
        return (zl - d + Zh) % Zh

    def x_at(d):
        return z * X + (x + d) % X

    def x_from(d):
        return (x - d + X) % X

    def t_of(yy, cc):
        return yy * 2 + cc

    def device(sp_at, tp_at):
        return {"sp": sp_at, "tp": tp_at}

    moves = [
        (k_one, stage.at[0]),
        (k_two, stage.at[1]),
        (q_one, stage.at[2]),
        (q_two, stage.at[3]),
        (values, value_stage),
        (out_weight, outw.at[j]),
        (down_weight, downw.at[pl.ds(pl.multiple_of(j * down_rows, down_rows), down_rows)]),
        (gate_weight, gate),
        (up_weight, up),
        (head_gain, head_scale),
        (norm_gain, norm_scale),
    ]
    moving = [
        pltpu.make_async_copy(src, dst, local_sem.at[i]) for i, (src, dst) in enumerate(moves)
    ]
    for copy in moving:
        copy.start()

    barrier = pltpu.get_barrier_semaphore()
    peers = [((s + d) % sp, t) for d in range(1, sp)]
    peers += [(s, (t + d) % T) for d in range(1, T)]
    peers += [(mate, (t + d) % T) for d in range(1, T)]
    for sp_at, tp_at in peers:
        pl.semaphore_signal(
            barrier, inc=1, device_id=device(sp_at, tp_at), device_id_type=pl.DeviceIdType.MESH
        )

    names = {}
    send_names = {}
    sends = []

    def slot(name):
        return names.setdefault(name, len(names))

    def send_slot(name):
        return send_names.setdefault(name, len(send_names))

    def send(src, dst, name, sp_at, tp_at, group=None):
        pltpu.make_async_remote_copy(
            src_ref=src, dst_ref=dst, send_sem=send_sem.at[send_slot(group or name)],
            recv_sem=recv_sem.at[slot(name)], device_id=device(sp_at, tp_at),
            device_id_type=pl.DeviceIdType.MESH,
        ).start()

    def wait(ref, send_at, recv_at):
        return pltpu.make_async_remote_copy(
            src_ref=ref, dst_ref=ref, send_sem=send_sem.at[send_at], recv_sem=recv_sem.at[recv_at],
            device_id=device(s, t), device_id_type=pl.DeviceIdType.MESH,
        )

    def arrive(ref, name, same=True):
        wait(ref, 0, slot(name)).wait_recv()
        if same:
            sends.append((ref, name))

    def sent(ref, name):
        wait(ref, send_slot(name), 0).wait_send()

    with scope("pack"):
        for copy in moving[:4]:
            copy.wait()
        size = stage.shape[2] // heads
        for i in range(heads):
            cols = slice(i * size, (i + 1) * size)
            k_pack[i] = jnp.concatenate([stage[0, :, cols], stage[1, :, cols]], axis=1)
            q_pack[i] = jnp.concatenate([stage[2, :, cols], stage[3, :, cols]], axis=1)
        for copy in moving[4:5]:
            copy.wait()
        value_size = v_all.shape[2]
        k_all[s] = k_pack[h]
        q_all[h] = q_pack[h]
        v_all[s] = value_stage[:, pl.ds(pl.multiple_of(h * value_size, value_size), value_size)]

    with scope("barrier"):
        pl.semaphore_wait(barrier, len(peers))

    targets = [other * G + (j + e) % G for e in range(G)]
    targets += [half * G + (j + e) % G for e in range(1, G)]
    for at in targets:
        send(k_pack.at[at % heads], k_all.at[s], "k", at, t)
    for d in range(1, heads):
        i = (h + d) % heads
        send(q_pack.at[i], q_all.at[h], "q", first + i, t)
    for at in targets:
        start = pl.multiple_of((at % heads) * value_size, value_size)
        send(value_stage.at[:, pl.ds(start, value_size)], v_all.at[s], "v", at, t)

    def rows_of(ref, count, k):
        size = ref.shape[1] // count
        return lambda zz, xx: ref.at[zz * X + xx, pl.ds(k * size, size)]

    def down_part(k):
        size = down_rows // C

        def at(zz, xx):
            start = pl.multiple_of((zz * X + xx) * down_rows + k * size, size)
            return downw.at[pl.ds(start, size)]

        return at

    def own_z(name, ref, group, last):
        for d in range(1, Zh):
            to = group + "_z" if last else (name, "z", d)
            send(ref(zl, x), ref(zl, x), to, z_at(d), t, group)

    def own_x(name, ref, group, last):
        for d in range(1, X):
            to = group + "_x" if last else (name, "x", d)
            send(ref(zl, x), ref(zl, x), to, x_at(d), t, group)

    def forward_x(name, ref, group):
        for d in range(1, Zh):
            block = ref(zl_from(d), x)
            arrive(block, (name, "z", d), False)
            for dx in range(1, X):
                send(block, block, group + "_rest", x_at(dx), t, group)

    def forward_z(name, ref, group):
        for d in range(1, X):
            block = ref(zl, x_from(d))
            arrive(block, (name, "x", d), False)
            for dz in range(1, Zh):
                send(block, block, group + "_rest", z_at(dz), t, group)

    def down(k):
        return "down%d" % k, down_part(k), "down"

    def out(k):
        return "out%d" % k, rows_of(outw, OC, k), "out"

    z_first = list(range(C - X_FIRST)) if C > X_FIRST else list(range(C))
    x_first = [k for k in range(C) if k not in z_first]

    nx = len(x_first)
    for copy in moving[5:7]:
        copy.wait()
    out_z_first = list(range(OC - OUT_X_FIRST)) if OC > OUT_X_FIRST else list(range(OC))
    out_x_first = [k for k in range(OC) if k not in out_z_first]
    for k in range(OC):
        own_z(*out(k), k in out_x_first)
        own_x(*out(k), k in out_z_first)
    for e, sp_at in enumerate((s, mate)):
        side = half if e == 0 else other
        for d in range(2):
            cc = c if d == 0 else 1 - c
            start = pl.multiple_of((side * 2 + cc) * quarter, quarter)
            src = residual.at[:, pl.ds(start, quarter)]
            if e or d:
                send(src, res.at[t], "res", sp_at, t_of(half, cc))
            else:
                k = slot("res")
                k_own = send_slot("res0")

                @pl.when(y == half)
                def _():
                    pltpu.make_async_copy(src, res.at[t], recv_sem.at[k]).start()

                @pl.when(y != half)
                def _():
                    pltpu.make_async_remote_copy(
                        src_ref=src, dst_ref=res.at[t], send_sem=send_sem.at[k_own],
                        recv_sem=recv_sem.at[k], device_id=device(s, t_of(half, cc)),
                        device_id_type=pl.DeviceIdType.MESH,
                    ).start()
    for k in x_first[:S0]:
        own_x(*down(k), False)

    with scope("wait_k"):
        arrive(q_all.at[pl.ds(0, heads - 1)], "q")
        arrive(k_all.at[pl.ds(0, sp - 1)], "k")
    pair = q_all.shape[2]
    head_size = pair // 2
    scale = head_size ** (-0.5)
    block_count = max(1, (sp * tokens) // 1024)
    block_sources = sp // block_count
    block_keys = block_sources * tokens
    lanes = lax.broadcasted_iota(jnp.int32, (1, pair), 1) // head_size

    def stack(q):
        return jnp.concatenate(
            [jnp.where(lanes == i, q, jnp.zeros_like(q)) for i in range(2)], axis=0
        )

    def maps(q):
        stacked = stack(q)

        def block(b, state):
            rows = pl.ds(b * block_sources, block_sources)
            scores = lax.dot_general(
                stacked, k_all[rows].reshape(block_keys, pair), ROWS_ROWS,
                preferred_element_type=f32,
            )
            newest = jnp.max(scores, axis=1, keepdims=True)
            newest = jnp.maximum(newest, state[0])
            shifted = jnp.exp((scores - newest) * scale)
            totals = jnp.sum(shifted, axis=1, keepdims=True)
            product = jnp.dot(
                shifted.astype(bf16), v_all[rows].reshape(block_keys, value_size),
                preferred_element_type=f32,
            )
            factor = jnp.exp((state[0] - newest) * scale)
            totals = totals + state[1] * factor
            product = product + state[2] * factor
            return newest, totals, product

        state = lax.fori_loop(
            0,
            block_count,
            block,
            (
                jnp.full((2 * tokens, 1), -jnp.inf, f32),
                jnp.zeros((2 * tokens, 1), f32),
                jnp.zeros((2 * tokens, value_size), f32),
            ),
        )
        return state[2] / state[1]

    moving[9].wait()
    head_cols = pl.ds(pl.multiple_of(h * value_size, value_size), value_size)
    turns = (*range(1, heads), 0)

    def attend(d, both):
        difference = both[:tokens] - lam[h] * both[tokens:]
        scaled = difference * lax.rsqrt(
            jnp.mean(difference * difference, axis=1, keepdims=True) + epsilon
        )
        att_out[d] = (scaled * head_scale[...]).astype(bf16)
        there = att.at[half, :, head_cols]
        i = (h + d) % heads
        send(att_out.at[d], there, "att_other", other * G + (first + i) % G, t)
        if d:
            send(att_out.at[d], there, "att_own", first + i, t)
        else:
            att[half, :, head_cols] = att_out[d]

    if block_count == 1:
        with scope("scores"):
            for d in turns:
                scores = lax.dot_general(
                    stack(q_all[(h + d) % heads]), k_all[...].reshape(block_keys, pair), ROWS_ROWS,
                    preferred_element_type=f32,
                )
                newest = jnp.max(scores, axis=1, keepdims=True)
                shifted = jnp.exp((scores - newest) * scale)
                totals_all[d] = jnp.sum(shifted, axis=1, keepdims=True)
                rounded_all[d] = shifted.astype(bf16)
        with scope("wait_v"):
            arrive(v_all.at[pl.ds(0, sp - 1)], "v")
        with scope("attention"):
            for d in turns:
                product = jnp.dot(
                    rounded_all[d], v_all[...].reshape(block_keys, value_size),
                    preferred_element_type=f32,
                )
                attend(d, product / totals_all[d])
    else:
        arrive(v_all.at[pl.ds(0, sp - 1)], "v")
        for d in turns:
            attend(d, maps(q_all[(h + d) % heads]))

    with scope("fwd_out"):
        for k in out_x_first:
            forward_z(*out(k))
        for k in out_z_first:
            forward_x(*out(k))
        for k in z_first[:S2]:
            own_z(*down(k), False)
    with scope("wait_att_own"):
        arrive(v_all.at[pl.ds(0, heads - 1)], "att_own")
    with scope("wait_att"):
        for k in x_first[S0 : S0 + S1]:
            own_x(*down(k), False)
        arrive(v_all.at[pl.ds(0, heads)], "att_other")
    with scope("wait_out"):
        size_out = outw.shape[1] // OC
        arrive(outw.at[pl.ds(0, X - 1), pl.ds(0, len(out_z_first) * size_out)], "out_x", False)
        if out_x_first:
            arrive(outw.at[pl.ds(0, Zh - 1), pl.ds(0, len(out_x_first) * size_out)], "out_z", False)
        arrive(outw.at[pl.ds(0, (X - 1) * (Zh - 1))], "out_rest", False)
    for k in z_first[S2:]:
        own_z(*down(k), False)
    for k in x_first[:S3]:
        own_z(*down(k), True)
    for k in x_first[S0 + S1 :]:
        own_x(*down(k), False)

    core_mate = t_of(y, 1 - c)
    width_out = att.shape[2]
    many = G // 2

    with scope("outproj"):
        rows_in = att[...].reshape(2 * tokens, width_out)

        def project(side):
            weight = outw[pl.ds(side * many, many)].reshape(quarter, width_out)
            return lax.dot_general(rows_in, weight, ROWS_ROWS, preferred_element_type=f32)

        core_out[0] = project(1 - c).astype(bf16)
        for d in (*range(1, Y), 0):
            lines = pl.ds(pl.multiple_of((y + d) % Y * tokens, tokens), tokens)
            send(core_out.at[0, lines], core_in.at[0, lines], ("p1c", d), s, core_mate, "p1c")
        own_sum[...] = project(c)
        for k in z_first:
            own_x(*down(k), True)
    def wait_core(d):
        lines = pl.ds(pl.multiple_of((y + d) % Y * tokens, tokens), tokens)
        arrive(core_in.at[0, lines], ("p1c", d), False)

    with scope("wait_p1c"):
        for d in range(1, Y):
            wait_core(d)

    def slot_rows(yy):
        return pl.ds(pl.multiple_of(yy * tokens, tokens), tokens)

    part = tokens // PIECES

    def slot_rows(yy, k):
        return pl.ds(pl.multiple_of(yy * tokens + k * part, part), part)

    with scope("sum_c"):
        for k in range(PIECES):
            for d in range(1, Y):
                yy = (y + d) % Y
                rows = slot_rows(yy, k)
                block = y_out.at[d - 1, pl.ds(k * part, part)]
                y_out[d - 1, k * part : (k + 1) * part] = (
                    own_sum[rows] + core_in[0, rows].astype(f32)
                ).astype(bf16)
                there = y_in.at[d - 1, pl.ds(k * part, part)]
                send(block, there, ("p1y", d, k), s, t_of(yy, c), "after")
    with scope("wait_res"):
        wait_core(0)
        arrive(res, "res", False)
    q_own = half * 2 + c
    q_mate = other * 2 + c

    def block_at(yy, q, k=None):
        cols = pl.ds(pl.multiple_of(q * quarter, quarter), quarter)
        rows = pl.ds(0, tokens) if k is None else pl.ds(k * part, part)
        return full.at[yy, rows, cols]

    with scope("sum_y"):
        residual_rows = res[...].reshape(tokens, quarter)
        own_cols = pl.ds(pl.multiple_of(q_own * quarter, quarter), quarter)
        for k in range(PIECES):
            rows = slot_rows(y, k)
            here = slice(k * part, (k + 1) * part)
            total = own_sum[rows] + core_in[0, rows].astype(f32)
            for d in range(1, Y):
                arrive(y_in.at[d - 1, pl.ds(k * part, part)], ("p1y", d, k), False)
                total = total + y_in[d - 1, here].astype(f32)
            total = total + residual_rows[here].astype(f32)
            full[y, here, own_cols] = total.astype(bf16)
            block = block_at(y, q_own, k)
            send(block, block, ("az", k), mate, t, "after")
            for d in range(1, Y):
                send(block, block, ("ay", d), s, t_of((y + d) % Y, c), "after")
        block = block_at(y, q_own)
        send(block, block, "ad_own", s, core_mate)
    with scope("bulk_a"):
        for k in x_first[S3:]:
            own_z(*down(k), True)
        for k in z_first[:3]:
            forward_x(*down(k))
        for k in x_first[: nx - 1]:
            forward_z(*down(k))

    width = hidden.shape[1]
    spans = [(at, min(512, width - at)) for at in range(0, width, 512)]
    side_size = 2 * quarter
    step = min(64, tokens)

    def scaled_rows(side):
        cols = pl.ds(pl.multiple_of(side * side_size, side_size), side_size)
        gain = norm_scale[:, cols]
        for yy in range(2):
            for at in range(0, tokens, step):
                stream = full[yy, at : at + step, cols].astype(f32)
                here = slice(yy * tokens + at, yy * tokens + at + step)
                squares[side, here] = jnp.sum(stream * stream, axis=1, keepdims=True)
                normed[side, here] = (stream * gain).astype(bf16)

    def products(side, at, n):
        rows = pl.ds(pl.multiple_of(side * side_size, side_size), side_size)
        left = normed[side]
        return (
            jnp.dot(left, gate[rows, at : at + n], preferred_element_type=f32),
            jnp.dot(left, up[rows, at : at + n], preferred_element_type=f32),
        )

    def early(at, n):
        gate_part, up_part = products(half, at, n)
        gate_sum[:, at : at + n] = gate_part
        up_sum[:, at : at + n] = up_part

    def pass_az(k):
        block = block_at(y, q_mate, k)
        arrive(block, ("az", k), False)
        for d in range(1, Y):
            send(block, block, ("ayz", d, k), s, t_of((y + d) % Y, c), "after")
        send(block, block, "ad_mate", s, core_mate)

    def pass_ayz(k):
        for d in range(1, Y):
            block = block_at((y - d + Y) % Y, q_mate, k)
            arrive(block, ("ayz", d, k), False)
            send(block, block, "ad_mate", s, core_mate)

    with scope("wait_az"):
        for k in range(PIECES // 2):
            pass_az(k)
    with scope("wait_ay"):
        for d in range(1, Y):
            block = block_at((y - d + Y) % Y, q_own)
            arrive(block, ("ay", d), False)
            send(block, block, "ad_own", s, core_mate)
    with scope("wait_az2"):
        for k in range(PIECES // 2, PIECES):
            pass_az(k)
    with scope("bulk_b"):
        for k in z_first[3:]:
            forward_x(*down(k))
        for k in x_first[nx - 1 :]:
            forward_z(*down(k))
    with scope("early"):
        arrive(full.at[0, :, pl.ds(0, side_size)], "ad_own")
        for copy in moving[7:9]:
            copy.wait()
        moving[10].wait()
        scaled_rows(half)
        for i, span in enumerate(spans):
            early(*span)
            if i < PIECES:
                pass_ayz(i)
        for k in range(len(spans), PIECES):
            pass_ayz(k)
    with scope("wait_ad"):
        arrive(full.at[0, :, pl.ds(0, side_size)], "ad_mate")

    with scope("norm"):
        scaled_rows(other)
        inverse[...] = lax.rsqrt(
            (squares[0] + squares[1]) * (1.0 / full.shape[2]) + epsilon
        )
    with scope("gateup"):
        for at, n in spans:
            gate_part, up_part = products(other, at, n)
            factor = inverse[...]
            gate_part = (gate_part + gate_sum[:, at : at + n]) * factor
            up_part = (up_part + up_sum[:, at : at + n]) * factor
            hidden[:, at : at + n] = (
                gate_part / (1.0 + jnp.exp(-gate_part)) * up_part
            ).astype(bf16)

    place = q_own * Y + y
    unit = prod.shape[2]
    half_unit = unit // 2
    size = down_rows // C
    staged = G == 4 and X == 2
    if staged:
        order = [j, zl * X + 1 - x, (1 - zl) * X + x, (1 - zl) * X + 1 - x]
    else:
        order = list(range(4))

    def lower(i):
        weight = downw[pl.ds(pl.multiple_of(order[i] * unit, unit), unit)]
        prod[i] = lax.dot_general(hidden[...], weight, ROWS_ROWS, preferred_element_type=f32)
        cols = pl.ds(pl.multiple_of((1 - c) * half_unit, half_unit), half_unit)
        lower_out[i] = prod[i, :, cols].astype(bf16)
        send(lower_out.at[i], lower_in.at[i], ("p2c", i), s, core_mate, "p2c")

    def to_owners(lo, n, name):
        units = pl.ds(lo, n)
        for i in range(lo, lo + n):
            arrive(lower_in.at[i], ("p2c", i), False)
        cols = pl.ds(pl.multiple_of(c * half_unit, half_unit), half_unit)
        for i in range(lo, lo + n):
            total = prod[i, :, cols] + lower_in[i].astype(f32)
            owner_out[:, :, i] = total.astype(bf16).reshape(2, T, piece, half_unit)
        for d in range(T):
            at = (t + d) % T
            send(owner_out.at[other, at, units], owner_in.at[place, units], name, mate, at)
        for d in range(1, T):
            at = (t + d) % T
            send(owner_out.at[half, at, units], owner_in.at[place, units], name, s, at)
        owner_in[place, units] = owner_out[half, t, units]

    def wait_x():
        if z_first:
            arrive(downw.at[pl.ds(0, len(z_first) * (X - 1) * size)], "down_x", False)

    def wait_z():
        if x_first:
            arrive(downw.at[pl.ds(0, nx * (Zh - 1) * size)], "down_z", False)

    def wait_rest():
        arrive(downw.at[pl.ds(0, (X - 1) * (Zh - 1) * down_rows)], "down_rest", False)

    if not staged:
        wait_x()
        wait_z()
        wait_rest()
    with scope("down_a"):
        lower(0)
        if staged:
            with scope("wait_x"):
                wait_x()
        lower(1)
        if staged:
            with scope("wait_z"):
                wait_z()
        lower(2)
    with scope("owners_a"):
        to_owners(0, 2, "p2o")
        to_owners(2, 1, "p3o")
    if staged:
        with scope("wait_rest"):
            wait_rest()
    with scope("down_b"):
        lower(3)
        to_owners(3, 1, "p4o")
    mine = pl.ds(pl.multiple_of(t * piece, piece), piece)

    def finish(lo, n, name):
        arrive(owner_in.at[pl.ds(0, 4 * Y - 1), pl.ds(lo, n)], name)
        for q in range(4):
            for i in range(lo, lo + n):
                start = (q // 2) * 4 * unit + order[i] * unit + (q % 2) * half_unit
                cols = pl.ds(pl.multiple_of(start, half_unit), half_unit)
                total = owner_in[q * Y, i].astype(f32)
                for k in range(1, Y):
                    total = total + owner_in[q * Y + k, i].astype(f32)
                result[:, cols] = (full[half, mine, cols].astype(f32) + total).astype(bf16)

    with scope("wait_p2o"):
        finish(0, 2, "p2o")
    with scope("wait_p3o"):
        finish(2, 1, "p3o")
    with scope("wait_p4o"):
        finish(3, 1, "p4o")
    with scope("wait_send"):
        for ref, name in sends:
            sent(ref, name)
        sent(outw.at[pl.ds(0, G - 1)], "out")
        sent(downw.at[pl.ds(0, (G - 1) * down_rows)], "down")
        assert 3 * (Y - 1) + 1 == 4
        sent(full.at[0], "after")
        sent(core_in.at[0], "p1c")
        sent(lower_in, "p2c")
        sent(res.at[pl.ds(0, 3)], "res")

        @pl.when(y != half)
        def _():
            sent(res.at[0], "res0")
    assert len(names) <= recv_sem.shape[0] and len(send_names) <= send_sem.shape[0]


def local(Z, X, T, *arrays):
    (residual, q_one, k_one, q_two, k_two, values, lam, head_gain, out_weight, norm_gain,
     gate_weight, up_weight, down_weight) = arrays
    sp = Z * X
    G = sp // 2
    bf16 = jnp.bfloat16
    heads = lam.shape[0]
    tokens, kw = k_one.shape
    vw = values.shape[1]
    pair = 2 * (kw // heads)
    vd = vw // heads
    piece, model = residual.shape
    quarter = model // 4
    width = gate_weight.shape[1]
    rows_down = down_weight.shape[0]
    C = max(1, min(CHUNKS, rows_down // 16))
    OC = max(1, min(OUT_CHUNKS, out_weight.shape[0] // 16))
    Y = T // 2
    vmem = pl.BlockSpec(memory_space=pltpu.VMEM)
    anywhere = pl.BlockSpec(memory_space=pl.ANY)
    smem = pl.BlockSpec(memory_space=pltpu.SMEM)
    Zh = Z // 2
    z_first = C - X_FIRST if C > X_FIRST else C
    received = 20 + 4 * PIECES + (OC + z_first) * (Zh - 1) + (C - z_first + OC) * (X - 1)
    return pl.pallas_call(
        functools.partial(kernel, Z, X, T, C, OC, heads),
        out_shape=pltpu.VMEM((piece, model), bf16),
        in_specs=[
            anywhere, anywhere, anywhere, anywhere, anywhere, anywhere, smem, anywhere, anywhere,
            anywhere,
            anywhere, anywhere, anywhere,
        ],
        out_specs=vmem,
        scratch_shapes=[
            pltpu.VMEM((4, tokens, kw), bf16),
            pltpu.VMEM((tokens, vw), bf16),
            pltpu.VMEM((heads, tokens, pair), bf16),
            pltpu.VMEM((heads, tokens, pair), bf16),
            pltpu.VMEM((heads, tokens, pair), bf16),
            pltpu.VMEM((sp, tokens, pair), bf16),
            pltpu.VMEM((sp, tokens, vd), bf16),
            pltpu.VMEM((G, out_weight.shape[0], vw), bf16),
            pltpu.VMEM((G * rows_down, width), bf16),
            pltpu.VMEM(gate_weight.shape, bf16),
            pltpu.VMEM(up_weight.shape, bf16),
            pltpu.VMEM((1, head_gain.shape[0]), jnp.float32),
            pltpu.VMEM((1, norm_gain.shape[0]), jnp.float32),
            pltpu.VMEM((heads, 2 * tokens, min(sp * tokens, 1024)), bf16),
            pltpu.VMEM((heads, 2 * tokens, 1), jnp.float32),
            pltpu.VMEM((heads, tokens, vd), bf16),
            pltpu.VMEM((2, tokens, vw), bf16),
            pltpu.VMEM((T, piece, quarter), bf16),
            pltpu.VMEM((1, 2 * tokens, quarter), bf16),
            pltpu.VMEM((1, 2 * tokens, quarter), bf16),
            pltpu.VMEM((4, 2 * tokens, model // 8), jnp.float32),
            pltpu.VMEM((4, 2 * tokens, model // 16), bf16),
            pltpu.VMEM((4, 2 * tokens, model // 16), bf16),
            pltpu.VMEM((Y - 1, tokens, quarter), bf16),
            pltpu.VMEM((Y - 1, tokens, quarter), bf16),
            pltpu.VMEM((2 * tokens, quarter), jnp.float32),
            pltpu.VMEM((2, tokens, model), bf16),
            pltpu.VMEM((2, 2 * tokens, model // 2), bf16),
            pltpu.VMEM((2, 2 * tokens, 1), jnp.float32),
            pltpu.VMEM((2 * tokens, 1), jnp.float32),
            pltpu.VMEM((2 * tokens, width), jnp.float32),
            pltpu.VMEM((2 * tokens, width), jnp.float32),
            pltpu.VMEM((2 * tokens, width), bf16),
            pltpu.VMEM((2, T, 4, piece, model // 16), bf16),
            pltpu.VMEM((4 * Y, 4, piece, model // 16), bf16),
            pltpu.SemaphoreType.DMA((11,)),
            pltpu.SemaphoreType.DMA((20,)),
            pltpu.SemaphoreType.DMA((received,)),
        ],
        compiler_params=pltpu.CompilerParams(
            collective_id=0, has_side_effects=True, vmem_limit_bytes=60 * 1024 * 1024
        ),
    )(
        residual, q_one, k_one, q_two, k_two, values, lam, head_gain.reshape(1, -1), out_weight,
        norm_gain.reshape(1, -1), gate_weight, up_weight, down_weight,
    )


def solution(mesh):
    Z, X = split_sp(mesh.shape["sp"])
    return jax.shard_map(
        functools.partial(local, Z, X, mesh.shape["tp"]),
        mesh=mesh,
        in_specs=(
            P(("sp", "tp"), None),
            P("sp", "tp"),
            P("sp", "tp"),
            P("sp", "tp"),
            P("sp", "tp"),
            P("sp", "tp"),
            P("tp"),
            P(),
            P("sp", "tp"),
            P(),
            P(None, "tp"),
            P(None, "tp"),
            P("sp", "tp"),
        ),
        out_specs=P(("sp", "tp"), None),
        check_vma=False,
    )
```

```python
import functools

import jax
import jax.numpy as jnp
from jax import lax
from jax.experimental import pallas as pl
from jax.experimental.pallas import tpu as pltpu
from jax.sharding import PartitionSpec as P

epsilon = 1e-06
ROWS_ROWS = (((1,), (1,)), ((), ()))
CHUNKS = 8
S4 = 0
S3 = 1
X_FIRST = 3
OUT_CHUNKS = 4
S0 = 1
S1 = 1
S2 = 5
OUT_X_FIRST = 0
PIECES = 4


def split_sp(size):
    inner = 1
    while (2 * inner) * (2 * inner) <= size:
        inner *= 2
    return size // inner, inner


def kernel(
    Z,
    X,
    T,
    C,
    OC,
    heads,
    residual,
    q_one,
    k_one,
    q_two,
    k_two,
    values,
    lam,
    head_gain,
    out_weight,
    norm_gain,
    gate_weight,
    up_weight,
    down_weight,
    result,
    stage,
    value_stage,
    q_pack,
    k_pack,
    q_all,
    k_all,
    v_all,
    outw,
    downw,
    gate,
    up,
    head_scale,
    norm_scale,
    weights,
    rounded_all,
    totals_all,
    att_out,
    att,
    res,
    core_out,
    core_in,
    prod,
    lower_out,
    lower_in,
    y_out,
    y_in,
    own_sum,
    full,
    normed,
    squares,
    inverse,
    gate_sum,
    up_sum,
    hidden,
    owner_out,
    owner_in,
    local_sem,
    send_sem,
    recv_sem,
):
    f32, bf16 = jnp.float32, jnp.bfloat16
    scope = jax.named_scope
    s = lax.axis_index("sp")
    t = lax.axis_index("tp")
    z, x = s // X, s % X
    sp = Z * X
    Zh = Z // 2
    G = Zh * X
    half = z // Zh
    other = 1 - half
    zl = z % Zh
    j = zl * X + x
    mate = other * G + j
    Y = T // 2
    y, c = t // 2, t % 2
    tokens = q_one.shape[0]
    piece = tokens // T
    down_rows = down_weight.shape[0]
    h = s % heads
    first = s - h
    quarter = full.shape[2] // 4

    def z_at(d):
        return (half * Zh + (zl + d) % Zh) * X + x

    def zl_from(d):
        return (zl - d + Zh) % Zh

    def x_at(d):
        return z * X + (x + d) % X

    def x_from(d):
        return (x - d + X) % X

    def t_of(yy, cc):
        return yy * 2 + cc

    def device(sp_at, tp_at):
        return {"sp": sp_at, "tp": tp_at}

    moves = [
        (k_one, stage.at[0]),
        (k_two, stage.at[1]),
        (q_one, stage.at[2]),
        (q_two, stage.at[3]),
        (values, value_stage),
        (out_weight, outw.at[j]),
        (down_weight, downw.at[pl.ds(pl.multiple_of(j * down_rows, down_rows), down_rows)]),
        (gate_weight, gate),
        (up_weight, up),
        (head_gain, head_scale),
        (norm_gain, norm_scale),
        (lam, weights),
    ]
    moving = [
        pltpu.make_async_copy(src, dst, local_sem.at[i]) for i, (src, dst) in enumerate(moves)
    ]
    for copy in moving:
        copy.start()

    barrier = pltpu.get_barrier_semaphore()
    peers = [((s + d) % sp, t) for d in range(1, sp)]
    peers += [(s, (t + d) % T) for d in range(1, T)]
    peers += [(mate, (t + d) % T) for d in range(1, T)]
    for sp_at, tp_at in peers:
        pl.semaphore_signal(
            barrier, inc=1, device_id=device(sp_at, tp_at), device_id_type=pl.DeviceIdType.MESH
        )

    names = {}
    send_names = {}
    sends = []

    def slot(name):
        return names.setdefault(name, len(names))

    def send_slot(name):
        return send_names.setdefault(name, len(send_names))

    def send(src, dst, name, sp_at, tp_at, group=None):
        pltpu.make_async_remote_copy(
            src_ref=src, dst_ref=dst, send_sem=send_sem.at[send_slot(group or name)],
            recv_sem=recv_sem.at[slot(name)], device_id=device(sp_at, tp_at),
            device_id_type=pl.DeviceIdType.MESH,
        ).start()

    def wait(ref, send_at, recv_at):
        return pltpu.make_async_remote_copy(
            src_ref=ref, dst_ref=ref, send_sem=send_sem.at[send_at], recv_sem=recv_sem.at[recv_at],
            device_id=device(s, t), device_id_type=pl.DeviceIdType.MESH,
        )

    def arrive(ref, name, same=True):
        wait(ref, 0, slot(name)).wait_recv()
        if same:
            sends.append((ref, name))

    def sent(ref, name):
        wait(ref, send_slot(name), 0).wait_send()

    with scope("pack"):
        for copy in moving[:4]:
            copy.wait()
        size = stage.shape[2] // heads
        for i in range(heads):
            cols = slice(i * size, (i + 1) * size)
            k_pack[i] = jnp.concatenate([stage[0, :, cols], stage[1, :, cols]], axis=1)
            q_pack[i] = jnp.concatenate([stage[2, :, cols], stage[3, :, cols]], axis=1)
        for copy in moving[4:5]:
            copy.wait()
        value_size = v_all.shape[2]
        k_all[s] = k_pack[h]
        q_all[h] = q_pack[h]
        v_all[s] = value_stage[:, pl.ds(pl.multiple_of(h * value_size, value_size), value_size)]

    with scope("barrier"):
        pl.semaphore_wait(barrier, len(peers))

    targets = [other * G + (j + e) % G for e in range(G)]
    targets += [half * G + (j + e) % G for e in range(1, G)]
    for at in targets:
        send(k_pack.at[at % heads], k_all.at[s], "k", at, t)
    for d in range(1, heads):
        i = (h + d) % heads
        send(q_pack.at[i], q_all.at[h], "q", first + i, t)
    for at in targets:
        start = pl.multiple_of((at % heads) * value_size, value_size)
        send(value_stage.at[:, pl.ds(start, value_size)], v_all.at[s], "v", at, t)

    def rows_of(ref, count, k):
        size = ref.shape[1] // count
        return lambda zz, xx: ref.at[zz * X + xx, pl.ds(k * size, size)]

    def down_part(k):
        size = down_rows // C

        def at(zz, xx):
            start = pl.multiple_of((zz * X + xx) * down_rows + k * size, size)
            return downw.at[pl.ds(start, size)]

        return at

    def own_z(name, ref, group, last):
        for d in range(1, Zh):
            to = group + "_z" if last else (name, "z", d)
            send(ref(zl, x), ref(zl, x), to, z_at(d), t, group)

    def own_x(name, ref, group, last):
        for d in range(1, X):
            to = group + "_x" if last else (name, "x", d)
            send(ref(zl, x), ref(zl, x), to, x_at(d), t, group)

    def forward_x(name, ref, group, late=False):
        for d in range(1, Zh):
            block = ref(zl_from(d), x)
            arrive(block, (name, "z", d), False)
            for dx in range(1, X):
                send(block, block, group + ("_late" if late else "_rest"), x_at(dx), t, group)

    def forward_z(name, ref, group, late=False):
        for d in range(1, X):
            block = ref(zl, x_from(d))
            arrive(block, (name, "x", d), False)
            for dz in range(1, Zh):
                send(block, block, group + ("_late" if late else "_rest"), z_at(dz), t, group)

    def down(k):
        return "down%d" % k, down_part(k), "down"

    def out(k):
        return "out%d" % k, rows_of(outw, OC, k), "out"

    z_first = list(range(C - X_FIRST)) if C > X_FIRST else list(range(C))
    x_first = [k for k in range(C) if k not in z_first]

    nx = len(x_first)
    for copy in moving[5:7]:
        copy.wait()
    out_z_first = list(range(OC - OUT_X_FIRST)) if OC > OUT_X_FIRST else list(range(OC))
    out_x_first = [k for k in range(OC) if k not in out_z_first]
    for k in range(OC):
        own_z(*out(k), k in out_x_first)
        own_x(*out(k), k in out_z_first)
    for e, sp_at in enumerate((s, mate)):
        side = half if e == 0 else other
        for d in range(2):
            cc = c if d == 0 else 1 - c
            start = pl.multiple_of((side * 2 + cc) * quarter, quarter)
            src = residual.at[:, pl.ds(start, quarter)]
            if e or d:
                send(src, res.at[t], "res", sp_at, t_of(half, cc))
            else:
                k = slot("res")
                k_own = send_slot("res0")

                @pl.when(y == half)
                def _():
                    pltpu.make_async_copy(src, res.at[t], recv_sem.at[k]).start()

                @pl.when(y != half)
                def _():
                    pltpu.make_async_remote_copy(
                        src_ref=src, dst_ref=res.at[t], send_sem=send_sem.at[k_own],
                        recv_sem=recv_sem.at[k], device_id=device(s, t_of(half, cc)),
                        device_id_type=pl.DeviceIdType.MESH,
                    ).start()
    for k in x_first[:S0]:
        own_x(*down(k), False)

    with scope("wait_k"):
        arrive(q_all.at[pl.ds(0, heads - 1)], "q")
        arrive(k_all.at[pl.ds(0, sp - 1)], "k")
    pair = q_all.shape[2]
    head_size = pair // 2
    scale = head_size ** (-0.5)
    block_count = max(1, (sp * tokens) // 1024)
    block_sources = sp // block_count
    block_keys = block_sources * tokens
    lanes = lax.broadcasted_iota(jnp.int32, (1, pair), 1) // head_size

    def stack(q):
        return jnp.concatenate(
            [jnp.where(lanes == i, q, jnp.zeros_like(q)) for i in range(2)], axis=0
        )

    def maps(q):
        stacked = stack(q)

        def block(b, state):
            rows = pl.ds(b * block_sources, block_sources)
            scores = lax.dot_general(
                stacked, k_all[rows].reshape(block_keys, pair), ROWS_ROWS,
                preferred_element_type=f32,
            )
            newest = jnp.max(scores, axis=1, keepdims=True)
            newest = jnp.maximum(newest, state[0])
            shifted = jnp.exp((scores - newest) * scale)
            totals = jnp.sum(shifted, axis=1, keepdims=True)
            product = jnp.dot(
                shifted.astype(bf16), v_all[rows].reshape(block_keys, value_size),
                preferred_element_type=f32,
            )
            factor = jnp.exp((state[0] - newest) * scale)
            totals = totals + state[1] * factor
            product = product + state[2] * factor
            return newest, totals, product

        state = lax.fori_loop(
            0,
            block_count,
            block,
            (
                jnp.full((2 * tokens, 1), -jnp.inf, f32),
                jnp.zeros((2 * tokens, 1), f32),
                jnp.zeros((2 * tokens, value_size), f32),
            ),
        )
        return state[2] / state[1]

    moving[9].wait()
    moving[11].wait()
    head_cols = pl.ds(pl.multiple_of(h * value_size, value_size), value_size)
    turns = (*range(1, heads), 0)

    def attend(d, both):
        difference = both[:tokens] - weights[h] * both[tokens:]
        scaled = difference * lax.rsqrt(
            jnp.mean(difference * difference, axis=1, keepdims=True) + epsilon
        )
        att_out[d] = (scaled * head_scale[...]).astype(bf16)
        there = att.at[half, :, head_cols]
        i = (h + d) % heads
        send(att_out.at[d], there, "att_other", other * G + (first + i) % G, t)
        if d:
            send(att_out.at[d], there, "att_own", first + i, t)
        else:
            att[half, :, head_cols] = att_out[d]

    if block_count == 1:
        with scope("scores"):
            for d in turns:
                scores = lax.dot_general(
                    stack(q_all[(h + d) % heads]), k_all[...].reshape(block_keys, pair), ROWS_ROWS,
                    preferred_element_type=f32,
                )
                newest = jnp.max(scores, axis=1, keepdims=True)
                shifted = jnp.exp((scores - newest) * scale)
                totals_all[d] = jnp.sum(shifted, axis=1, keepdims=True)
                rounded_all[d] = shifted.astype(bf16)
        with scope("wait_v"):
            arrive(v_all.at[pl.ds(0, sp - 1)], "v")
        with scope("attention"):
            for d in turns:
                product = jnp.dot(
                    rounded_all[d], v_all[...].reshape(block_keys, value_size),
                    preferred_element_type=f32,
                )
                attend(d, product / totals_all[d])
    else:
        arrive(v_all.at[pl.ds(0, sp - 1)], "v")
        for d in turns:
            attend(d, maps(q_all[(h + d) % heads]))

    with scope("fwd_out"):
        for k in out_x_first:
            forward_z(*out(k))
        for k in out_z_first:
            forward_x(*out(k))
        for k in z_first[:S2]:
            own_z(*down(k), False)
    with scope("wait_att_own"):
        arrive(v_all.at[pl.ds(0, heads - 1)], "att_own")
    with scope("wait_att"):
        for k in x_first[S0 : S0 + S1]:
            own_x(*down(k), False)
        arrive(v_all.at[pl.ds(0, heads)], "att_other")
    with scope("wait_out"):
        size_out = outw.shape[1] // OC
        arrive(outw.at[pl.ds(0, X - 1), pl.ds(0, len(out_z_first) * size_out)], "out_x", False)
        if out_x_first:
            arrive(outw.at[pl.ds(0, Zh - 1), pl.ds(0, len(out_x_first) * size_out)], "out_z", False)
        arrive(outw.at[pl.ds(0, (X - 1) * (Zh - 1))], "out_rest", False)
    for k in z_first[S2:]:
        own_z(*down(k), False)
    for k in x_first[:S3]:
        own_z(*down(k), True)
    for k in x_first[:S4]:
        forward_z(*down(k), 2 * k >= C)
    for k in x_first[S0 + S1 :]:
        own_x(*down(k), False)

    core_mate = t_of(y, 1 - c)
    width_out = att.shape[2]
    many = G // 2

    with scope("outproj"):
        rows_in = att[...].reshape(2 * tokens, width_out)

        def project(side):
            weight = outw[pl.ds(side * many, many)].reshape(quarter, width_out)
            return lax.dot_general(rows_in, weight, ROWS_ROWS, preferred_element_type=f32)

        core_out[0] = project(1 - c).astype(bf16)
        for d in (*range(1, Y), 0):
            lines = pl.ds(pl.multiple_of((y + d) % Y * tokens, tokens), tokens)
            send(core_out.at[0, lines], core_in.at[0, lines], ("p1c", d), s, core_mate, "p1c")
        own_sum[...] = project(c)
        for k in z_first:
            own_x(*down(k), True)
    def wait_core(d):
        lines = pl.ds(pl.multiple_of((y + d) % Y * tokens, tokens), tokens)
        arrive(core_in.at[0, lines], ("p1c", d), False)

    with scope("wait_p1c"):
        for d in range(1, Y):
            wait_core(d)

    def slot_rows(yy):
        return pl.ds(pl.multiple_of(yy * tokens, tokens), tokens)

    part = tokens // PIECES

    def slot_rows(yy, k):
        return pl.ds(pl.multiple_of(yy * tokens + k * part, part), part)

    with scope("sum_c"):
        for k in range(PIECES):
            for d in range(1, Y):
                yy = (y + d) % Y
                rows = slot_rows(yy, k)
                block = y_out.at[d - 1, pl.ds(k * part, part)]
                y_out[d - 1, k * part : (k + 1) * part] = (
                    own_sum[rows] + core_in[0, rows].astype(f32)
                ).astype(bf16)
                there = y_in.at[d - 1, pl.ds(k * part, part)]
                send(block, there, ("p1y", d, k), s, t_of(yy, c), "after")
    with scope("wait_res"):
        wait_core(0)
        arrive(res, "res", False)
    q_own = half * 2 + c
    q_mate = other * 2 + c

    def block_at(yy, q, k=None):
        cols = pl.ds(pl.multiple_of(q * quarter, quarter), quarter)
        rows = pl.ds(0, tokens) if k is None else pl.ds(k * part, part)
        return full.at[yy, rows, cols]

    with scope("sum_y"):
        residual_rows = res[...].reshape(tokens, quarter)
        own_cols = pl.ds(pl.multiple_of(q_own * quarter, quarter), quarter)
        for k in range(PIECES):
            rows = slot_rows(y, k)
            here = slice(k * part, (k + 1) * part)
            total = own_sum[rows] + core_in[0, rows].astype(f32)
            for d in range(1, Y):
                arrive(y_in.at[d - 1, pl.ds(k * part, part)], ("p1y", d, k), False)
                total = total + y_in[d - 1, here].astype(f32)
            total = total + residual_rows[here].astype(f32)
            full[y, here, own_cols] = total.astype(bf16)
            block = block_at(y, q_own, k)
            send(block, block, ("az", k), mate, t, "after")
            for d in range(1, Y):
                send(block, block, ("ay", d), s, t_of((y + d) % Y, c), "after")
        block = block_at(y, q_own)
        send(block, block, "ad_own", s, core_mate)
    with scope("bulk_a"):
        for k in x_first[S3:]:
            own_z(*down(k), True)
        for k in z_first[:3]:
            forward_x(*down(k), 2 * k >= C)
        for k in x_first[S4 : nx - 1]:
            forward_z(*down(k), 2 * k >= C)

    width = hidden.shape[1]
    spans = [(at, min(512, width - at)) for at in range(0, width, 512)]
    side_size = 2 * quarter
    step = min(64, tokens)

    def scaled_rows(side, start, size):
        cols = pl.ds(pl.multiple_of(side * side_size + start, quarter), size)
        inner = pl.ds(start if isinstance(start, int) else pl.multiple_of(start, quarter), size)
        gain = norm_scale[:, cols]
        for yy in range(2):
            for at in range(0, tokens, step):
                stream = full[yy, at : at + step, cols].astype(f32)
                here = slice(yy * tokens + at, yy * tokens + at + step)
                part = jnp.sum(stream * stream, axis=1, keepdims=True)
                squares[here] = part if size == side_size else squares[here] + part
                normed[side, here, inner] = (stream * gain).astype(bf16)

    def products(side, start, size, at, n):
        rows = pl.ds(pl.multiple_of(side * side_size + start, quarter), size)
        inner = pl.ds(start if isinstance(start, int) else pl.multiple_of(start, quarter), size)
        left = normed[side, :, inner]
        return (
            jnp.dot(left, gate[rows, at : at + n], preferred_element_type=f32),
            jnp.dot(left, up[rows, at : at + n], preferred_element_type=f32),
        )

    def early(at, n):
        gate_part, up_part = products(half, 0, side_size, at, n)
        gate_sum[:, at : at + n] = gate_part
        up_sum[:, at : at + n] = up_part

    def pass_az(k):
        block = block_at(y, q_mate, k)
        arrive(block, ("az", k), False)
        for d in range(1, Y):
            send(block, block, ("ayz", d, k), s, t_of((y + d) % Y, c), "after")
        send(block, block, "ad_mate", s, core_mate)

    def pass_ayz(k):
        for d in range(1, Y):
            block = block_at((y - d + Y) % Y, q_mate, k)
            arrive(block, ("ayz", d, k), False)
            send(block, block, "ad_mate", s, core_mate)

    with scope("wait_az"):
        for k in range(PIECES // 2):
            pass_az(k)
    with scope("wait_ay"):
        for d in range(1, Y):
            block = block_at((y - d + Y) % Y, q_own)
            arrive(block, ("ay", d), False)
            send(block, block, "ad_own", s, core_mate)
    with scope("wait_az2"):
        for k in range(PIECES // 2, PIECES):
            pass_az(k)
    with scope("bulk_b"):
        for k in z_first[3:]:
            forward_x(*down(k), 2 * k >= C)
        for k in x_first[nx - 1 :]:
            forward_z(*down(k), 2 * k >= C)
    with scope("early"):
        arrive(full.at[0, :, pl.ds(0, side_size)], "ad_own")
        for copy in moving[7:9]:
            copy.wait()
        moving[10].wait()
        scaled_rows(half, 0, side_size)
        for i, span in enumerate(spans):
            early(*span)
            if i < PIECES:
                pass_ayz(i)
        for k in range(len(spans), PIECES):
            pass_ayz(k)
    with scope("middle"):
        scaled_rows(other, c * quarter, quarter)
        for at, n in spans:
            gate_part, up_part = products(other, c * quarter, quarter, at, n)
            gate_sum[:, at : at + n] += gate_part
            up_sum[:, at : at + n] += up_part
    with scope("wait_ad"):
        arrive(full.at[0, :, pl.ds(0, side_size)], "ad_mate")

    with scope("norm"):
        scaled_rows(other, (1 - c) * quarter, quarter)
        inverse[...] = lax.rsqrt(squares[...] * (1.0 / full.shape[2]) + epsilon)
    with scope("gateup"):
        for at, n in spans:
            gate_part, up_part = products(other, (1 - c) * quarter, quarter, at, n)
            factor = inverse[...]
            gate_part = (gate_part + gate_sum[:, at : at + n]) * factor
            up_part = (up_part + up_sum[:, at : at + n]) * factor
            hidden[:, at : at + n] = (
                gate_part / (1.0 + jnp.exp(-gate_part)) * up_part
            ).astype(bf16)

    place = q_own * Y + y
    unit = prod.shape[2]
    half_unit = unit // 2
    size = down_rows // C
    staged = G == 4 and X == 2
    if staged:
        order = [j, zl * X + 1 - x, (1 - zl) * X + x, (1 - zl) * X + 1 - x]
    else:
        order = list(range(4))

    def lower(i):
        weight = downw[pl.ds(pl.multiple_of(order[i] * unit, unit), unit)]
        prod[i] = lax.dot_general(hidden[...], weight, ROWS_ROWS, preferred_element_type=f32)
        cols = pl.ds(pl.multiple_of((1 - c) * half_unit, half_unit), half_unit)
        lower_out[i] = prod[i, :, cols].astype(bf16)
        send(lower_out.at[i], lower_in.at[i], ("p2c", i), s, core_mate, "p2c")

    def to_owners(lo, n, name):
        units = pl.ds(lo, n)
        for i in range(lo, lo + n):
            arrive(lower_in.at[i], ("p2c", i), False)
        cols = pl.ds(pl.multiple_of(c * half_unit, half_unit), half_unit)
        for i in range(lo, lo + n):
            total = prod[i, :, cols] + lower_in[i].astype(f32)
            owner_out[:, :, i] = total.astype(bf16).reshape(2, T, piece, half_unit)
        for d in range(T):
            at = (t + d) % T
            send(owner_out.at[other, at, units], owner_in.at[place, units], name, mate, at)
        for d in range(1, T):
            at = (t + d) % T
            send(owner_out.at[half, at, units], owner_in.at[place, units], name, s, at)
        owner_in[place, units] = owner_out[half, t, units]

    def wait_x():
        if z_first:
            arrive(downw.at[pl.ds(0, len(z_first) * (X - 1) * size)], "down_x", False)

    def wait_z():
        if x_first:
            arrive(downw.at[pl.ds(0, nx * (Zh - 1) * size)], "down_z", False)

    def wait_rest(late):
        count = C // 2 if late else C - C // 2
        if count:
            rows = pl.ds(0, (X - 1) * (Zh - 1) * count * size)
            arrive(downw.at[rows], "down_late" if late else "down_rest", False)

    if not staged:
        wait_x()
        wait_z()
        wait_rest(False)
        wait_rest(True)
    with scope("down_a"):
        lower(0)
        if staged:
            with scope("wait_x"):
                wait_x()
        lower(1)
        if staged:
            with scope("wait_z"):
                wait_z()
        to_owners(0, 1, "p1o")
        lower(2)
    with scope("owners_a"):
        to_owners(1, 1, "p2o")
        to_owners(2, 1, "p3o")
    start = order[3] * unit
    for side in range(2):
        if staged:
            with scope("wait_rest"):
                wait_rest(bool(side))
        with scope("down_b"):
            weight = downw[pl.ds(pl.multiple_of(start + side * half_unit, half_unit), half_unit)]
            product = lax.dot_general(hidden[...], weight, ROWS_ROWS, preferred_element_type=f32)
            prod[3, :, side * half_unit : (side + 1) * half_unit] = product

            @pl.when(c != side)
            def _():
                lower_out[3] = product.astype(bf16)
                send(lower_out.at[3], lower_in.at[3], ("p2c", 3), s, core_mate, "p2c")

    with scope("owners_b"):
        to_owners(3, 1, "p4o")
    mine = pl.ds(pl.multiple_of(t * piece, piece), piece)

    def finish(lo, n, name):
        arrive(owner_in.at[pl.ds(0, 4 * Y - 1), pl.ds(lo, n)], name)
        for q in range(4):
            for i in range(lo, lo + n):
                start = (q // 2) * 4 * unit + order[i] * unit + (q % 2) * half_unit
                cols = pl.ds(pl.multiple_of(start, half_unit), half_unit)
                total = owner_in[q * Y, i].astype(f32)
                for k in range(1, Y):
                    total = total + owner_in[q * Y + k, i].astype(f32)
                result[:, cols] = (full[half, mine, cols].astype(f32) + total).astype(bf16)

    with scope("wait_p2o"):
        finish(0, 1, "p1o")
        finish(1, 1, "p2o")
    with scope("wait_p3o"):
        finish(2, 1, "p3o")
    with scope("wait_p4o"):
        finish(3, 1, "p4o")
    with scope("wait_send"):
        for ref, name in sends:
            sent(ref, name)
        sent(outw.at[pl.ds(0, G - 1)], "out")
        sent(downw.at[pl.ds(0, (G - 1) * down_rows)], "down")
        assert 3 * (Y - 1) + 1 == 4
        sent(full.at[0], "after")
        sent(core_in.at[0], "p1c")
        sent(lower_in, "p2c")
        sent(res.at[pl.ds(0, 3)], "res")

        @pl.when(y != half)
        def _():
            sent(res.at[0], "res0")
    assert len(names) <= recv_sem.shape[0] and len(send_names) <= send_sem.shape[0]


def local(Z, X, T, *arrays):
    (residual, q_one, k_one, q_two, k_two, values, lam, head_gain, out_weight, norm_gain,
     gate_weight, up_weight, down_weight) = arrays
    sp = Z * X
    G = sp // 2
    bf16 = jnp.bfloat16
    heads = lam.shape[0]
    tokens, kw = k_one.shape
    vw = values.shape[1]
    pair = 2 * (kw // heads)
    vd = vw // heads
    piece, model = residual.shape
    quarter = model // 4
    width = gate_weight.shape[1]
    rows_down = down_weight.shape[0]
    C = max(1, min(CHUNKS, rows_down // 16))
    OC = max(1, min(OUT_CHUNKS, out_weight.shape[0] // 16))
    Y = T // 2
    vmem = pl.BlockSpec(memory_space=pltpu.VMEM)
    anywhere = pl.BlockSpec(memory_space=pl.ANY)
    Zh = Z // 2
    z_first = C - X_FIRST if C > X_FIRST else C
    received = 20 + 4 * PIECES + (OC + z_first) * (Zh - 1) + (C - z_first + OC) * (X - 1)
    return pl.pallas_call(
        functools.partial(kernel, Z, X, T, C, OC, heads),
        out_shape=pltpu.VMEM((piece, model), bf16),
        in_specs=[
            anywhere, anywhere, anywhere, anywhere, anywhere, anywhere, anywhere, anywhere, anywhere,
            anywhere,
            anywhere, anywhere, anywhere,
        ],
        out_specs=vmem,
        scratch_shapes=[
            pltpu.VMEM((4, tokens, kw), bf16),
            pltpu.VMEM((tokens, vw), bf16),
            pltpu.VMEM((heads, tokens, pair), bf16),
            pltpu.VMEM((heads, tokens, pair), bf16),
            pltpu.VMEM((heads, tokens, pair), bf16),
            pltpu.VMEM((sp, tokens, pair), bf16),
            pltpu.VMEM((sp, tokens, vd), bf16),
            pltpu.VMEM((G, out_weight.shape[0], vw), bf16),
            pltpu.VMEM((G * rows_down, width), bf16),
            pltpu.VMEM(gate_weight.shape, bf16),
            pltpu.VMEM(up_weight.shape, bf16),
            pltpu.VMEM((1, head_gain.shape[0]), jnp.float32),
            pltpu.VMEM((1, norm_gain.shape[0]), jnp.float32),
            pltpu.SMEM(lam.shape, jnp.float32),
            pltpu.VMEM((heads, 2 * tokens, min(sp * tokens, 1024)), bf16),
            pltpu.VMEM((heads, 2 * tokens, 1), jnp.float32),
            pltpu.VMEM((heads, tokens, vd), bf16),
            pltpu.VMEM((2, tokens, vw), bf16),
            pltpu.VMEM((T, piece, quarter), bf16),
            pltpu.VMEM((1, 2 * tokens, quarter), bf16),
            pltpu.VMEM((1, 2 * tokens, quarter), bf16),
            pltpu.VMEM((4, 2 * tokens, model // 8), jnp.float32),
            pltpu.VMEM((4, 2 * tokens, model // 16), bf16),
            pltpu.VMEM((4, 2 * tokens, model // 16), bf16),
            pltpu.VMEM((Y - 1, tokens, quarter), bf16),
            pltpu.VMEM((Y - 1, tokens, quarter), bf16),
            pltpu.VMEM((2 * tokens, quarter), jnp.float32),
            pltpu.VMEM((2, tokens, model), bf16),
            pltpu.VMEM((2, 2 * tokens, model // 2), bf16),
            pltpu.VMEM((2 * tokens, 1), jnp.float32),
            pltpu.VMEM((2 * tokens, 1), jnp.float32),
            pltpu.VMEM((2 * tokens, width), jnp.float32),
            pltpu.VMEM((2 * tokens, width), jnp.float32),
            pltpu.VMEM((2 * tokens, width), bf16),
            pltpu.VMEM((2, T, 4, piece, model // 16), bf16),
            pltpu.VMEM((4 * Y, 4, piece, model // 16), bf16),
            pltpu.SemaphoreType.DMA((12,)),
            pltpu.SemaphoreType.DMA((21,)),
            pltpu.SemaphoreType.DMA((received,)),
        ],
        compiler_params=pltpu.CompilerParams(
            collective_id=0, has_side_effects=True, vmem_limit_bytes=60 * 1024 * 1024
        ),
    )(
        residual, q_one, k_one, q_two, k_two, values, lam, head_gain.reshape(1, -1), out_weight,
        norm_gain.reshape(1, -1), gate_weight, up_weight, down_weight,
    )


def solution(mesh):
    Z, X = split_sp(mesh.shape["sp"])
    return jax.shard_map(
        functools.partial(local, Z, X, mesh.shape["tp"]),
        mesh=mesh,
        in_specs=(
            P(("sp", "tp"), None),
            P("sp", "tp"),
            P("sp", "tp"),
            P("sp", "tp"),
            P("sp", "tp"),
            P("sp", "tp"),
            P("tp"),
            P(),
            P("sp", "tp"),
            P(),
            P(None, "tp"),
            P(None, "tp"),
            P("sp", "tp"),
        ),
        out_specs=P(("sp", "tp"), None),
        check_vma=False,
    )
```

```python
import functools

import jax
import jax.numpy as jnp
from jax import lax
from jax.experimental import pallas as pl
from jax.experimental.pallas import tpu as pltpu
from jax.sharding import PartitionSpec as P

epsilon = 1e-06
ROWS_ROWS = (((1,), (1,)), ((), ()))
CHUNKS = 8
S4 = 0
S3 = 1
X_FIRST = 3
OUT_CHUNKS = 4
S0 = 1
S1 = 1
S2 = 5
OUT_X_FIRST = 0
PIECES = 8


def split_sp(size):
    inner = 1
    while (2 * inner) * (2 * inner) <= size:
        inner *= 2
    return size // inner, inner


def kernel(
    Z,
    X,
    T,
    C,
    OC,
    heads,
    residual,
    q_one,
    k_one,
    q_two,
    k_two,
    values,
    lam,
    head_gain,
    out_weight,
    norm_gain,
    gate_weight,
    up_weight,
    down_weight,
    result,
    stage,
    value_stage,
    q_pack,
    k_pack,
    q_all,
    k_all,
    v_all,
    outw,
    downw,
    gate,
    up,
    head_scale,
    norm_scale,
    weights,
    rounded_all,
    totals_all,
    att_out,
    att,
    res,
    core_out,
    core_in,
    prod,
    lower_out,
    lower_in,
    y_out,
    y_in,
    own_sum,
    full,
    normed,
    squares,
    inverse,
    gate_sum,
    up_sum,
    hidden,
    owner_out,
    owner_in,
    local_sem,
    send_sem,
    recv_sem,
):
    f32, bf16 = jnp.float32, jnp.bfloat16
    scope = jax.named_scope
    s = lax.axis_index("sp")
    t = lax.axis_index("tp")
    z, x = s // X, s % X
    sp = Z * X
    Zh = Z // 2
    G = Zh * X
    half = z // Zh
    other = 1 - half
    zl = z % Zh
    j = zl * X + x
    mate = other * G + j
    Y = T // 2
    y, c = t // 2, t % 2
    tokens = q_one.shape[0]
    piece = tokens // T
    down_rows = down_weight.shape[0]
    h = s % heads
    first = s - h
    quarter = full.shape[2] // 4

    def z_at(d):
        return (half * Zh + (zl + d) % Zh) * X + x

    def zl_from(d):
        return (zl - d + Zh) % Zh

    def x_at(d):
        return z * X + (x + d) % X

    def x_from(d):
        return (x - d + X) % X

    def t_of(yy, cc):
        return yy * 2 + cc

    def device(sp_at, tp_at):
        return {"sp": sp_at, "tp": tp_at}

    moves = [
        (k_one, stage.at[0]),
        (k_two, stage.at[1]),
        (q_one, stage.at[2]),
        (q_two, stage.at[3]),
        (values, value_stage),
        (out_weight, outw.at[j]),
        (down_weight, downw.at[pl.ds(pl.multiple_of(j * down_rows, down_rows), down_rows)]),
        (gate_weight, gate),
        (up_weight, up),
        (head_gain, head_scale),
        (norm_gain, norm_scale),
        (lam, weights),
    ]
    moving = [
        pltpu.make_async_copy(src, dst, local_sem.at[i]) for i, (src, dst) in enumerate(moves)
    ]
    for copy in moving:
        copy.start()

    barrier = pltpu.get_barrier_semaphore()
    peers = [((s + d) % sp, t) for d in range(1, sp)]
    peers += [(s, (t + d) % T) for d in range(1, T)]
    peers += [(mate, (t + d) % T) for d in range(1, T)]
    for sp_at, tp_at in peers:
        pl.semaphore_signal(
            barrier, inc=1, device_id=device(sp_at, tp_at), device_id_type=pl.DeviceIdType.MESH
        )

    names = {}
    send_names = {}
    sends = []

    def slot(name):
        return names.setdefault(name, len(names))

    def send_slot(name):
        return send_names.setdefault(name, len(send_names))

    def send(src, dst, name, sp_at, tp_at, group=None):
        pltpu.make_async_remote_copy(
            src_ref=src, dst_ref=dst, send_sem=send_sem.at[send_slot(group or name)],
            recv_sem=recv_sem.at[slot(name)], device_id=device(sp_at, tp_at),
            device_id_type=pl.DeviceIdType.MESH,
        ).start()

    def wait(ref, send_at, recv_at):
        return pltpu.make_async_remote_copy(
            src_ref=ref, dst_ref=ref, send_sem=send_sem.at[send_at], recv_sem=recv_sem.at[recv_at],
            device_id=device(s, t), device_id_type=pl.DeviceIdType.MESH,
        )

    def arrive(ref, name, same=True):
        wait(ref, 0, slot(name)).wait_recv()
        if same:
            sends.append((ref, name))

    def sent(ref, name):
        wait(ref, send_slot(name), 0).wait_send()

    with scope("pack"):
        for copy in moving[:4]:
            copy.wait()
        size = stage.shape[2] // heads
        for i in range(heads):
            cols = slice(i * size, (i + 1) * size)
            k_pack[i] = jnp.concatenate([stage[0, :, cols], stage[1, :, cols]], axis=1)
            q_pack[i] = jnp.concatenate([stage[2, :, cols], stage[3, :, cols]], axis=1)
        for copy in moving[4:5]:
            copy.wait()
        value_size = v_all.shape[2]
        k_all[s] = k_pack[h]
        q_all[h] = q_pack[h]
        v_all[s] = value_stage[:, pl.ds(pl.multiple_of(h * value_size, value_size), value_size)]

    with scope("barrier"):
        pl.semaphore_wait(barrier, len(peers))

    targets = [other * G + (j + e) % G for e in range(G)]
    targets += [half * G + (j + e) % G for e in range(1, G)]
    for at in targets:
        send(k_pack.at[at % heads], k_all.at[s], "k", at, t)
    for d in range(1, heads):
        i = (h + d) % heads
        send(q_pack.at[i], q_all.at[h], "q", first + i, t)
    for at in targets:
        start = pl.multiple_of((at % heads) * value_size, value_size)
        send(value_stage.at[:, pl.ds(start, value_size)], v_all.at[s], "v", at, t)

    def rows_of(ref, count, k):
        size = ref.shape[1] // count
        return lambda zz, xx: ref.at[zz * X + xx, pl.ds(k * size, size)]

    def down_part(k):
        size = down_rows // C

        def at(zz, xx):
            start = pl.multiple_of((zz * X + xx) * down_rows + k * size, size)
            return downw.at[pl.ds(start, size)]

        return at

    def own_z(name, ref, group, last):
        for d in range(1, Zh):
            to = group + "_z" if last else (name, "z", d)
            send(ref(zl, x), ref(zl, x), to, z_at(d), t, group)

    def own_x(name, ref, group, last):
        for d in range(1, X):
            to = group + "_x" if last else (name, "x", d)
            send(ref(zl, x), ref(zl, x), to, x_at(d), t, group)

    def forward_x(name, ref, group, late=False):
        for d in range(1, Zh):
            block = ref(zl_from(d), x)
            arrive(block, (name, "z", d), False)
            for dx in range(1, X):
                send(block, block, group + ("_late" if late else "_rest"), x_at(dx), t, group)

    def forward_z(name, ref, group, late=False):
        for d in range(1, X):
            block = ref(zl, x_from(d))
            arrive(block, (name, "x", d), False)
            for dz in range(1, Zh):
                send(block, block, group + ("_late" if late else "_rest"), z_at(dz), t, group)

    def down(k):
        return "down%d" % k, down_part(k), "down"

    def out(k):
        return "out%d" % k, rows_of(outw, OC, k), "out"

    z_first = list(range(C - X_FIRST)) if C > X_FIRST else list(range(C))
    x_first = [k for k in range(C) if k not in z_first]

    nx = len(x_first)
    for copy in moving[5:7]:
        copy.wait()
    out_z_first = list(range(OC - OUT_X_FIRST)) if OC > OUT_X_FIRST else list(range(OC))
    out_x_first = [k for k in range(OC) if k not in out_z_first]
    for k in range(OC):
        own_z(*out(k), k in out_x_first)
        own_x(*out(k), k in out_z_first)
    for e, sp_at in enumerate((s, mate)):
        side = half if e == 0 else other
        for d in range(2):
            cc = c if d == 0 else 1 - c
            start = pl.multiple_of((side * 2 + cc) * quarter, quarter)
            src = residual.at[:, pl.ds(start, quarter)]
            if e or d:
                send(src, res.at[t], "res", sp_at, t_of(half, cc))
            else:
                k = slot("res")
                k_own = send_slot("res0")

                @pl.when(y == half)
                def _():
                    pltpu.make_async_copy(src, res.at[t], recv_sem.at[k]).start()

                @pl.when(y != half)
                def _():
                    pltpu.make_async_remote_copy(
                        src_ref=src, dst_ref=res.at[t], send_sem=send_sem.at[k_own],
                        recv_sem=recv_sem.at[k], device_id=device(s, t_of(half, cc)),
                        device_id_type=pl.DeviceIdType.MESH,
                    ).start()
    for k in x_first[:S0]:
        own_x(*down(k), False)

    with scope("wait_k"):
        arrive(q_all.at[pl.ds(0, heads - 1)], "q")
        arrive(k_all.at[pl.ds(0, sp - 1)], "k")
    pair = q_all.shape[2]
    head_size = pair // 2
    scale = head_size ** (-0.5)
    block_count = max(1, (sp * tokens) // 1024)
    block_sources = sp // block_count
    block_keys = block_sources * tokens
    lanes = lax.broadcasted_iota(jnp.int32, (1, pair), 1) // head_size

    def stack(q):
        return jnp.concatenate(
            [jnp.where(lanes == i, q, jnp.zeros_like(q)) for i in range(2)], axis=0
        )

    def maps(q):
        stacked = stack(q)

        def block(b, state):
            rows = pl.ds(b * block_sources, block_sources)
            scores = lax.dot_general(
                stacked, k_all[rows].reshape(block_keys, pair), ROWS_ROWS,
                preferred_element_type=f32,
            )
            newest = jnp.max(scores, axis=1, keepdims=True)
            newest = jnp.maximum(newest, state[0])
            shifted = jnp.exp((scores - newest) * scale)
            totals = jnp.sum(shifted, axis=1, keepdims=True)
            product = jnp.dot(
                shifted.astype(bf16), v_all[rows].reshape(block_keys, value_size),
                preferred_element_type=f32,
            )
            factor = jnp.exp((state[0] - newest) * scale)
            totals = totals + state[1] * factor
            product = product + state[2] * factor
            return newest, totals, product

        state = lax.fori_loop(
            0,
            block_count,
            block,
            (
                jnp.full((2 * tokens, 1), -jnp.inf, f32),
                jnp.zeros((2 * tokens, 1), f32),
                jnp.zeros((2 * tokens, value_size), f32),
            ),
        )
        return state[2] / state[1]

    moving[9].wait()
    moving[11].wait()
    head_cols = pl.ds(pl.multiple_of(h * value_size, value_size), value_size)
    turns = (*range(1, heads), 0)

    def attend(d, both):
        difference = both[:tokens] - weights[h] * both[tokens:]
        scaled = difference * lax.rsqrt(
            jnp.mean(difference * difference, axis=1, keepdims=True) + epsilon
        )
        att_out[d] = (scaled * head_scale[...]).astype(bf16)
        there = att.at[half, :, head_cols]
        i = (h + d) % heads
        send(att_out.at[d], there, "att_other", other * G + (first + i) % G, t)
        if d:
            send(att_out.at[d], there, "att_own", first + i, t)
        else:
            att[half, :, head_cols] = att_out[d]

    if block_count == 1:
        with scope("scores"):
            for d in turns:
                scores = lax.dot_general(
                    stack(q_all[(h + d) % heads]), k_all[...].reshape(block_keys, pair), ROWS_ROWS,
                    preferred_element_type=f32,
                )
                newest = jnp.max(scores, axis=1, keepdims=True)
                shifted = jnp.exp((scores - newest) * scale)
                totals_all[d] = jnp.sum(shifted, axis=1, keepdims=True)
                rounded_all[d] = shifted.astype(bf16)
        with scope("wait_v"):
            arrive(v_all.at[pl.ds(0, sp - 1)], "v")
        with scope("attention"):
            for d in turns:
                product = jnp.dot(
                    rounded_all[d], v_all[...].reshape(block_keys, value_size),
                    preferred_element_type=f32,
                )
                attend(d, product / totals_all[d])
    else:
        arrive(v_all.at[pl.ds(0, sp - 1)], "v")
        for d in turns:
            attend(d, maps(q_all[(h + d) % heads]))

    with scope("fwd_out"):
        for k in out_x_first:
            forward_z(*out(k))
        for k in out_z_first:
            forward_x(*out(k))
        for k in z_first[:S2]:
            own_z(*down(k), False)
    with scope("wait_att_own"):
        arrive(v_all.at[pl.ds(0, heads - 1)], "att_own")
    with scope("wait_att"):
        for k in x_first[S0 : S0 + S1]:
            own_x(*down(k), False)
        arrive(v_all.at[pl.ds(0, heads)], "att_other")
    with scope("wait_out"):
        size_out = outw.shape[1] // OC
        arrive(outw.at[pl.ds(0, X - 1), pl.ds(0, len(out_z_first) * size_out)], "out_x", False)
        if out_x_first:
            arrive(outw.at[pl.ds(0, Zh - 1), pl.ds(0, len(out_x_first) * size_out)], "out_z", False)
        arrive(outw.at[pl.ds(0, (X - 1) * (Zh - 1))], "out_rest", False)
    for k in z_first[S2:]:
        own_z(*down(k), False)
    for k in x_first[:S3]:
        own_z(*down(k), True)
    for k in x_first[:S4]:
        forward_z(*down(k), 2 * k >= C)
    for k in x_first[S0 + S1 :]:
        own_x(*down(k), False)

    core_mate = t_of(y, 1 - c)
    width_out = att.shape[2]
    many = G // 2

    with scope("outproj"):
        rows_in = att[...].reshape(2 * tokens, width_out)

        def project(side):
            weight = outw[pl.ds(side * many, many)].reshape(quarter, width_out)
            return lax.dot_general(rows_in, weight, ROWS_ROWS, preferred_element_type=f32)

        core_out[0] = project(1 - c).astype(bf16)
        for d in (*range(1, Y), 0):
            lines = pl.ds(pl.multiple_of((y + d) % Y * tokens, tokens), tokens)
            send(core_out.at[0, lines], core_in.at[0, lines], ("p1c", d), s, core_mate, "p1c")
        own_sum[...] = project(c)
        for k in z_first:
            own_x(*down(k), True)
    def wait_core(d):
        lines = pl.ds(pl.multiple_of((y + d) % Y * tokens, tokens), tokens)
        arrive(core_in.at[0, lines], ("p1c", d), False)

    with scope("wait_p1c"):
        for d in range(1, Y):
            wait_core(d)

    def slot_rows(yy):
        return pl.ds(pl.multiple_of(yy * tokens, tokens), tokens)

    part = tokens // PIECES

    def slot_rows(yy, k):
        return pl.ds(pl.multiple_of(yy * tokens + k * part, part), part)

    with scope("sum_c"):
        for k in range(PIECES):
            for d in range(1, Y):
                yy = (y + d) % Y
                rows = slot_rows(yy, k)
                block = y_out.at[d - 1, pl.ds(k * part, part)]
                y_out[d - 1, k * part : (k + 1) * part] = (
                    own_sum[rows] + core_in[0, rows].astype(f32)
                ).astype(bf16)
                there = y_in.at[d - 1, pl.ds(k * part, part)]
                send(block, there, ("p1y", d, k), s, t_of(yy, c), "after")
    with scope("wait_res"):
        wait_core(0)
        arrive(res, "res", False)
    q_own = half * 2 + c
    q_mate = other * 2 + c

    def block_at(yy, q, k=None):
        cols = pl.ds(pl.multiple_of(q * quarter, quarter), quarter)
        rows = pl.ds(0, tokens) if k is None else pl.ds(k * part, part)
        return full.at[yy, rows, cols]

    with scope("sum_y"):
        residual_rows = res[...].reshape(tokens, quarter)
        own_cols = pl.ds(pl.multiple_of(q_own * quarter, quarter), quarter)
        for k in range(PIECES):
            rows = slot_rows(y, k)
            here = slice(k * part, (k + 1) * part)
            total = own_sum[rows] + core_in[0, rows].astype(f32)
            for d in range(1, Y):
                arrive(y_in.at[d - 1, pl.ds(k * part, part)], ("p1y", d, k), False)
                total = total + y_in[d - 1, here].astype(f32)
            total = total + residual_rows[here].astype(f32)
            full[y, here, own_cols] = total.astype(bf16)
            block = block_at(y, q_own, k)
            send(block, block, ("az", k), mate, t, "after")
            for d in range(1, Y):
                send(block, block, ("ay", d), s, t_of((y + d) % Y, c), "after")
        block = block_at(y, q_own)
        send(block, block, "ad_own", s, core_mate)
    with scope("bulk_a"):
        for k in x_first[S3:]:
            own_z(*down(k), True)
        for k in z_first[:3]:
            forward_x(*down(k), 2 * k >= C)
        for k in x_first[S4 : nx - 1]:
            forward_z(*down(k), 2 * k >= C)

    width = hidden.shape[1]
    spans = [(at, min(512, width - at)) for at in range(0, width, 512)]
    side_size = 2 * quarter
    step = min(64, tokens)

    def scaled_rows(side, start, size):
        cols = pl.ds(pl.multiple_of(side * side_size + start, quarter), size)
        inner = pl.ds(start if isinstance(start, int) else pl.multiple_of(start, quarter), size)
        gain = norm_scale[:, cols]
        for yy in range(2):
            for at in range(0, tokens, step):
                stream = full[yy, at : at + step, cols].astype(f32)
                here = slice(yy * tokens + at, yy * tokens + at + step)
                part = jnp.sum(stream * stream, axis=1, keepdims=True)
                squares[here] = part if size == side_size else squares[here] + part
                normed[side, here, inner] = (stream * gain).astype(bf16)

    def products(side, start, size, at, n):
        rows = pl.ds(pl.multiple_of(side * side_size + start, quarter), size)
        inner = pl.ds(start if isinstance(start, int) else pl.multiple_of(start, quarter), size)
        left = normed[side, :, inner]
        return (
            jnp.dot(left, gate[rows, at : at + n], preferred_element_type=f32),
            jnp.dot(left, up[rows, at : at + n], preferred_element_type=f32),
        )

    def early(at, n):
        gate_part, up_part = products(half, 0, side_size, at, n)
        gate_sum[:, at : at + n] = gate_part
        up_sum[:, at : at + n] = up_part

    def pass_az(k):
        block = block_at(y, q_mate, k)
        arrive(block, ("az", k), False)
        for d in range(1, Y):
            send(block, block, ("ayz", d, k), s, t_of((y + d) % Y, c), "after")
        send(block, block, "ad_mate", s, core_mate)

    def pass_ayz(k):
        for d in range(1, Y):
            block = block_at((y - d + Y) % Y, q_mate, k)
            arrive(block, ("ayz", d, k), False)
            send(block, block, "ad_mate", s, core_mate)

    with scope("wait_az"):
        for k in range(PIECES // 2):
            pass_az(k)
    with scope("wait_ay"):
        for d in range(1, Y):
            block = block_at((y - d + Y) % Y, q_own)
            arrive(block, ("ay", d), False)
            send(block, block, "ad_own", s, core_mate)
    with scope("wait_az2"):
        for k in range(PIECES // 2, PIECES):
            pass_az(k)
    with scope("bulk_b"):
        for k in z_first[3:]:
            forward_x(*down(k), 2 * k >= C)
        for k in x_first[nx - 1 :]:
            forward_z(*down(k), 2 * k >= C)
    with scope("early"):
        arrive(full.at[0, :, pl.ds(0, side_size)], "ad_own")
        for copy in moving[7:9]:
            copy.wait()
        moving[10].wait()
        scaled_rows(half, 0, side_size)
        for i, span in enumerate(spans):
            early(*span)
            if i < PIECES:
                pass_ayz(i)
        for k in range(len(spans), PIECES):
            pass_ayz(k)
    with scope("middle"):
        scaled_rows(other, c * quarter, quarter)
        for at, n in spans:
            gate_part, up_part = products(other, c * quarter, quarter, at, n)
            gate_sum[:, at : at + n] += gate_part
            up_sum[:, at : at + n] += up_part
    with scope("wait_ad"):
        arrive(full.at[0, :, pl.ds(0, side_size)], "ad_mate")

    with scope("norm"):
        scaled_rows(other, (1 - c) * quarter, quarter)
        inverse[...] = lax.rsqrt(squares[...] * (1.0 / full.shape[2]) + epsilon)
    with scope("gateup"):
        for at, n in spans:
            gate_part, up_part = products(other, (1 - c) * quarter, quarter, at, n)
            factor = inverse[...]
            gate_part = (gate_part + gate_sum[:, at : at + n]) * factor
            up_part = (up_part + up_sum[:, at : at + n]) * factor
            hidden[:, at : at + n] = (
                gate_part / (1.0 + jnp.exp(-gate_part)) * up_part
            ).astype(bf16)

    place = q_own * Y + y
    unit = prod.shape[2]
    half_unit = unit // 2
    size = down_rows // C
    staged = G == 4 and X == 2
    if staged:
        order = [j, zl * X + 1 - x, (1 - zl) * X + x, (1 - zl) * X + 1 - x]
    else:
        order = list(range(4))

    def lower(i):
        weight = downw[pl.ds(pl.multiple_of(order[i] * unit, unit), unit)]
        prod[i] = lax.dot_general(hidden[...], weight, ROWS_ROWS, preferred_element_type=f32)
        cols = pl.ds(pl.multiple_of((1 - c) * half_unit, half_unit), half_unit)
        lower_out[i] = prod[i, :, cols].astype(bf16)
        send(lower_out.at[i], lower_in.at[i], ("p2c", i), s, core_mate, "p2c")

    def to_owners(lo, n, name):
        units = pl.ds(lo, n)
        for i in range(lo, lo + n):
            arrive(lower_in.at[i], ("p2c", i), False)
        cols = pl.ds(pl.multiple_of(c * half_unit, half_unit), half_unit)
        for i in range(lo, lo + n):
            total = prod[i, :, cols] + lower_in[i].astype(f32)
            owner_out[:, :, i] = total.astype(bf16).reshape(2, T, piece, half_unit)
        for d in range(T):
            at = (t + d) % T
            send(owner_out.at[other, at, units], owner_in.at[place, units], name, mate, at)
        for d in range(1, T):
            at = (t + d) % T
            send(owner_out.at[half, at, units], owner_in.at[place, units], name, s, at)
        owner_in[place, units] = owner_out[half, t, units]

    def wait_x():
        if z_first:
            arrive(downw.at[pl.ds(0, len(z_first) * (X - 1) * size)], "down_x", False)

    def wait_z():
        if x_first:
            arrive(downw.at[pl.ds(0, nx * (Zh - 1) * size)], "down_z", False)

    def wait_rest(late):
        count = C // 2 if late else C - C // 2
        if count:
            rows = pl.ds(0, (X - 1) * (Zh - 1) * count * size)
            arrive(downw.at[rows], "down_late" if late else "down_rest", False)

    if not staged:
        wait_x()
        wait_z()
        wait_rest(False)
        wait_rest(True)
    with scope("down_a"):
        lower(0)
        if staged:
            with scope("wait_x"):
                wait_x()
        lower(1)
        if staged:
            with scope("wait_z"):
                wait_z()
        to_owners(0, 1, "p1o")
        lower(2)
    with scope("owners_a"):
        to_owners(1, 1, "p2o")
        to_owners(2, 1, "p3o")
    start = order[3] * unit
    for side in range(2):
        if staged:
            with scope("wait_rest"):
                wait_rest(bool(side))
        with scope("down_b"):
            weight = downw[pl.ds(pl.multiple_of(start + side * half_unit, half_unit), half_unit)]
            product = lax.dot_general(hidden[...], weight, ROWS_ROWS, preferred_element_type=f32)
            prod[3, :, side * half_unit : (side + 1) * half_unit] = product

            @pl.when(c != side)
            def _():
                lower_out[3] = product.astype(bf16)
                send(lower_out.at[3], lower_in.at[3], ("p2c", 3), s, core_mate, "p2c")

    with scope("owners_b"):
        to_owners(3, 1, "p4o")
    mine = pl.ds(pl.multiple_of(t * piece, piece), piece)

    def finish(lo, n, name):
        arrive(owner_in.at[pl.ds(0, 4 * Y - 1), pl.ds(lo, n)], name)
        for q in range(4):
            for i in range(lo, lo + n):
                start = (q // 2) * 4 * unit + order[i] * unit + (q % 2) * half_unit
                cols = pl.ds(pl.multiple_of(start, half_unit), half_unit)
                total = owner_in[q * Y, i].astype(f32)
                for k in range(1, Y):
                    total = total + owner_in[q * Y + k, i].astype(f32)
                result[:, cols] = (full[half, mine, cols].astype(f32) + total).astype(bf16)

    with scope("wait_p2o"):
        finish(0, 1, "p1o")
        finish(1, 1, "p2o")
    with scope("wait_p3o"):
        finish(2, 1, "p3o")
    with scope("wait_p4o"):
        finish(3, 1, "p4o")
    with scope("wait_send"):
        for ref, name in sends:
            sent(ref, name)
        sent(outw.at[pl.ds(0, G - 1)], "out")
        sent(downw.at[pl.ds(0, (G - 1) * down_rows)], "down")
        assert 3 * (Y - 1) + 1 == 4
        sent(full.at[0], "after")
        sent(core_in.at[0], "p1c")
        sent(lower_in, "p2c")
        sent(res.at[pl.ds(0, 3)], "res")

        @pl.when(y != half)
        def _():
            sent(res.at[0], "res0")
    assert len(names) <= recv_sem.shape[0] and len(send_names) <= send_sem.shape[0]


def local(Z, X, T, *arrays):
    (residual, q_one, k_one, q_two, k_two, values, lam, head_gain, out_weight, norm_gain,
     gate_weight, up_weight, down_weight) = arrays
    sp = Z * X
    G = sp // 2
    bf16 = jnp.bfloat16
    heads = lam.shape[0]
    tokens, kw = k_one.shape
    vw = values.shape[1]
    pair = 2 * (kw // heads)
    vd = vw // heads
    piece, model = residual.shape
    quarter = model // 4
    width = gate_weight.shape[1]
    rows_down = down_weight.shape[0]
    C = max(1, min(CHUNKS, rows_down // 16))
    OC = max(1, min(OUT_CHUNKS, out_weight.shape[0] // 16))
    Y = T // 2
    vmem = pl.BlockSpec(memory_space=pltpu.VMEM)
    anywhere = pl.BlockSpec(memory_space=pl.ANY)
    Zh = Z // 2
    z_first = C - X_FIRST if C > X_FIRST else C
    received = 21 + 3 * PIECES + (OC + z_first) * (Zh - 1) + (C - z_first + OC) * (X - 1)
    return pl.pallas_call(
        functools.partial(kernel, Z, X, T, C, OC, heads),
        out_shape=pltpu.VMEM((piece, model), bf16),
        in_specs=[
            anywhere, anywhere, anywhere, anywhere, anywhere, anywhere, anywhere, anywhere, anywhere,
            anywhere,
            anywhere, anywhere, anywhere,
        ],
        out_specs=vmem,
        scratch_shapes=[
            pltpu.VMEM((4, tokens, kw), bf16),
            pltpu.VMEM((tokens, vw), bf16),
            pltpu.VMEM((heads, tokens, pair), bf16),
            pltpu.VMEM((heads, tokens, pair), bf16),
            pltpu.VMEM((heads, tokens, pair), bf16),
            pltpu.VMEM((sp, tokens, pair), bf16),
            pltpu.VMEM((sp, tokens, vd), bf16),
            pltpu.VMEM((G, out_weight.shape[0], vw), bf16),
            pltpu.VMEM((G * rows_down, width), bf16),
            pltpu.VMEM(gate_weight.shape, bf16),
            pltpu.VMEM(up_weight.shape, bf16),
            pltpu.VMEM((1, head_gain.shape[0]), jnp.float32),
            pltpu.VMEM((1, norm_gain.shape[0]), jnp.float32),
            pltpu.SMEM(lam.shape, jnp.float32),
            pltpu.VMEM((heads, 2 * tokens, min(sp * tokens, 1024)), bf16),
            pltpu.VMEM((heads, 2 * tokens, 1), jnp.float32),
            pltpu.VMEM((heads, tokens, vd), bf16),
            pltpu.VMEM((2, tokens, vw), bf16),
            pltpu.VMEM((T, piece, quarter), bf16),
            pltpu.VMEM((1, 2 * tokens, quarter), bf16),
            pltpu.VMEM((1, 2 * tokens, quarter), bf16),
            pltpu.VMEM((4, 2 * tokens, model // 8), jnp.float32),
            pltpu.VMEM((4, 2 * tokens, model // 16), bf16),
            pltpu.VMEM((4, 2 * tokens, model // 16), bf16),
            pltpu.VMEM((Y - 1, tokens, quarter), bf16),
            pltpu.VMEM((Y - 1, tokens, quarter), bf16),
            pltpu.VMEM((2 * tokens, quarter), jnp.float32),
            pltpu.VMEM((2, tokens, model), bf16),
            pltpu.VMEM((2, 2 * tokens, model // 2), bf16),
            pltpu.VMEM((2 * tokens, 1), jnp.float32),
            pltpu.VMEM((2 * tokens, 1), jnp.float32),
            pltpu.VMEM((2 * tokens, width), jnp.float32),
            pltpu.VMEM((2 * tokens, width), jnp.float32),
            pltpu.VMEM((2 * tokens, width), bf16),
            pltpu.VMEM((2, T, 4, piece, model // 16), bf16),
            pltpu.VMEM((4 * Y, 4, piece, model // 16), bf16),
            pltpu.SemaphoreType.DMA((12,)),
            pltpu.SemaphoreType.DMA((21,)),
            pltpu.SemaphoreType.DMA((received,)),
        ],
        compiler_params=pltpu.CompilerParams(
            collective_id=0, has_side_effects=True, vmem_limit_bytes=60 * 1024 * 1024
        ),
    )(
        residual, q_one, k_one, q_two, k_two, values, lam, head_gain.reshape(1, -1), out_weight,
        norm_gain.reshape(1, -1), gate_weight, up_weight, down_weight,
    )


def solution(mesh):
    Z, X = split_sp(mesh.shape["sp"])
    return jax.shard_map(
        functools.partial(local, Z, X, mesh.shape["tp"]),
        mesh=mesh,
        in_specs=(
            P(("sp", "tp"), None),
            P("sp", "tp"),
            P("sp", "tp"),
            P("sp", "tp"),
            P("sp", "tp"),
            P("sp", "tp"),
            P("tp"),
            P(),
            P("sp", "tp"),
            P(),
            P(None, "tp"),
            P(None, "tp"),
            P("sp", "tp"),
        ),
        out_specs=P(("sp", "tp"), None),
        check_vma=False,
    )
```
